32 devices in a mesh: rep: 2 (over x), fs: 8 (over z, y), tp: 2 (over core).
Axes of the slice: x: 2, y: 2, z: 4, core: 2. Of those that a mesh axis runs over, the one named last changes fastest.
Arguments:
- tokens: bfloat16 [10240, 2048], P(('rep', 'fs', 'tp')), may hold values from -6 to 6
- mix_gain: float32 [2048], replicated, may hold values from 0.1 to 1.9
- w_bgate: bfloat16 [2048, 2048], P('fs', 'tp'), may hold values from -0.125 to 0.125
- w_cgate: bfloat16 [2048, 2048], P('fs', 'tp'), may hold values from -0.125 to 0.125
- w_value: bfloat16 [2048, 2048], P('fs', 'tp'), may hold values from -0.125 to 0.125
- conv_taps: float32 [3, 2048], replicated, may hold values from -3 to 3
- w_mixout: bfloat16 [2048, 2048], P('tp', 'fs'), may hold values from -0.125 to 0.125
- mlp_gain: float32 [2048], replicated, may hold values from 0.1 to 1.9
- w_gate: bfloat16 [2048, 2816], P('fs', 'tp'), may hold values from -0.125 to 0.125
- w_up: bfloat16 [2048, 2816], P('fs', 'tp'), may hold values from -0.125 to 0.125
- w_down: bfloat16 [2816, 2048], P('tp', 'fs'), may hold values from -0.109375 to 0.109375
Outputs:
- block_out: bfloat16 [10240, 2048], P(('rep', 'fs', 'tp'))
The draws below stay inside these ranges and needn't reach their ends.
All inputs are finite; a program needn't handle non-finite values.
Results may differ from the reference program's by a relative error of at most 0.0085.
Values may be sent and summed in bfloat16 or wider, within the bound.
A program may use at most 128 MiB of HBM per device.

```python
import jax
import jax.numpy as jnp
from jax import lax

D = 2048
FF = 2816
LENGTH = 640
TOKENS = 10240
N_TP = 2


def block_scale(key, extent, split, least, top_value):
    level, own = 1.0, jax.random.fold_in(key, 6)
    for dim, blocks in split:
        steps = jnp.exp(jax.random.uniform(jax.random.fold_in(own, dim), (blocks,), jnp.float32, least / len(split), top_value / len(split)))
        level = level * jnp.repeat(steps, extent[dim] // blocks).reshape([-1 if axis == dim else 1 for axis in range(len(extent))])
    return level


def centred(own_key, extent, width, bound, cuts=(), dtype=jnp.bfloat16):
    drawn = jax.random.normal(own_key, extent, jnp.float32) * width
    if len(cuts) > 0:
        drawn = block_scale(own_key, extent, cuts, -0.22, 0.18) * drawn
    return jnp.clip(drawn, min=-bound, max=bound).astype(dtype)


def setup_inputs(seed: int = 0) -> dict:
    key_of = jax.random.split(jax.random.key(seed), 12)
    tokens = centred(key_of[0], (TOKENS, D), 1.0, 6.0, ((0, 32),))
    mix_gain = jnp.clip(1.0 + 0.18 * jax.random.normal(key_of[1], (D,), jnp.float32), 0.1, 1.9)
    w_bgate = centred(key_of[2], (D, D), D ** -0.5, 0.125, ((0, 8), (1, 2)))
    w_cgate = centred(key_of[3], (D, D), D ** -0.5, 0.125, ((0, 8), (1, 2)))
    w_value = centred(key_of[4], (D, D), D ** -0.5, 0.125, ((0, 8), (1, 2)))
    conv_taps = centred(key_of[5], (3, D), 0.6, 3.0, (), jnp.float32)
    w_mixout = centred(key_of[6], (D, D), D ** -0.5, 0.125, ((0, 2), (1, 8)))
    mlp_gain = jnp.clip(1.0 + 0.18 * jax.random.normal(key_of[7], (D,), jnp.float32), 0.1, 1.9)
    w_gate = centred(key_of[8], (D, FF), D ** -0.5, 0.125, ((0, 8), (1, 2)))
    w_up = centred(key_of[9], (D, FF), D ** -0.5, 0.125, ((0, 8), (1, 2)))
    w_down = centred(key_of[10], (FF, D), FF ** -0.5, 0.109375, ((0, 2), (1, 8)))
    return {"tokens": tokens, "mix_gain": mix_gain, "w_bgate": w_bgate, "w_cgate": w_cgate, "w_value": w_value, "conv_taps": conv_taps, "w_mixout": w_mixout, "mlp_gain": mlp_gain, "w_gate": w_gate, "w_up": w_up, "w_down": w_down}


def rms_scale(matrix, gain):
    values = matrix.astype(jnp.float32)
    factor = lax.rsqrt(lax.optimization_barrier(jnp.mean(values * values, axis=-1, keepdims=True)) + 1e-06)
    return values * factor * gain.astype(jnp.float32)

def causal_taps(mixed, filters):
    length = mixed.shape[-2]
    widths = [(0, 0)] * (mixed.ndim - 2) + [(2, 0), (0, 0)]
    padded = jnp.pad(mixed, widths)
    return filters[0] * padded[..., 0:length, :] + filters[1] * padded[..., 1:length + 1, :] + filters[2] * padded[..., 2:length + 2, :]

def split_sum(left, right):
    portion = left.shape[1] // N_TP
    running = jnp.zeros((left.shape[0], right.shape[1]), jnp.float32)
    for member in range(N_TP):
        partial_out = jnp.dot(left[:, member * portion:(member + 1) * portion], right[member * portion:(member + 1) * portion], preferred_element_type=jnp.float32)
        partial_out = lax.optimization_barrier(partial_out.astype(jnp.bfloat16))
        running = running + partial_out.astype(jnp.float32)
    return running

def reference(tokens, mix_gain, w_bgate, w_cgate, w_value, conv_taps, w_mixout, mlp_gain, w_gate, w_up, w_down):
    normed = rms_scale(tokens, mix_gain).astype(jnp.bfloat16)
    b_proj = jnp.dot(normed, w_bgate, preferred_element_type=jnp.float32).astype(jnp.bfloat16)
    c_proj = jnp.dot(normed, w_cgate, preferred_element_type=jnp.float32).astype(jnp.bfloat16)
    u_proj = jnp.dot(normed, w_value, preferred_element_type=jnp.float32).astype(jnp.bfloat16)
    mixed_in = c_proj.astype(jnp.float32) * u_proj.astype(jnp.float32)
    mixed_in = mixed_in.reshape(TOKENS // LENGTH, LENGTH, D)
    convolved = causal_taps(mixed_in, conv_taps).reshape(TOKENS, D)
    gated = (b_proj.astype(jnp.float32) * convolved).astype(jnp.bfloat16)
    residual = tokens.astype(jnp.float32) + split_sum(gated, w_mixout)
    normed_two = rms_scale(residual, mlp_gain).astype(jnp.bfloat16)
    gate = jnp.dot(normed_two, w_gate, preferred_element_type=jnp.float32)
    up_value = jnp.dot(normed_two, w_up, preferred_element_type=jnp.float32)
    hidden = (jax.nn.silu(gate) * up_value).astype(jnp.bfloat16)
    return (residual + 0.5 * split_sum(hidden, w_down)).astype(jnp.bfloat16)
```

```python
import functools

import jax
import jax.numpy as jnp
from jax import lax
from jax.experimental import pallas as pl
from jax.experimental.pallas import tpu as pltpu
from jax.sharding import PartitionSpec as P


def rms_scale(matrix, gain):
    values = matrix.astype(jnp.float32)
    factor = lax.rsqrt(jnp.mean(values * values, axis=-1, keepdims=True) + 1e-06)
    return values * factor * gain


def causal_taps(mixed, filters):
    length = mixed.shape[-2]
    padded = jnp.pad(mixed, [(2, 0), (0, 0)])
    return (
        filters[0] * padded[0:length]
        + filters[1] * padded[1 : length + 1]
        + filters[2] * padded[2 : length + 2]
    )


def swap(array, axis):
    return lax.ppermute(array, axis, [(0, 1), (1, 0)])


def half(array, axis, part):
    size = array.shape[axis] // 2
    return lax.dynamic_slice_in_dim(array, part * size, size, axis)


def build(n_fs):
    ring = [(i, (i + 2) % n_fs) for i in range(n_fs)]
    pair = [(i, i ^ 1) for i in range(n_fs)]
    steps = n_fs // 2

    def ring_first(block):
        blocks = []
        for step in range(steps):
            blocks += [block, lax.ppermute(block, "fs", pair)]
            if step < steps - 1:
                block = lax.ppermute(block, "fs", ring)
        return blocks

    def pair_first(block):
        mate = lax.ppermute(block, "fs", pair)
        blocks = []
        for step in range(steps):
            blocks += [block, mate]
            if step < steps - 1:
                block = lax.ppermute(block, "fs", ring)
                mate = lax.ppermute(mate, "fs", ring)
        return blocks

    def on_device(
        tokens, mix_gain, w_bgate, w_cgate, w_value, conv_taps, w_mixout, mlp_gain, w_gate, w_up, w_down
    ):
        rep, fs, tp = (lax.axis_index(name) for name in ("rep", "fs", "tp"))
        width = tokens.shape[1] // n_fs

        def arrival_order(array):
            order = [((fs ^ j) - 2 * s + n_fs) % n_fs for s in range(steps) for j in range(2)]
            return jnp.concatenate(
                [lax.dynamic_slice_in_dim(array, k * width, width, array.ndim - 1) for k in order],
                axis=-1,
            )

        def global_order(array):
            places = []
            for k in range(n_fs):
                j = (fs ^ k) & 1
                places.append((((fs ^ j) - k + n_fs) % n_fs) + j)
            return jnp.concatenate(
                [lax.dynamic_slice_in_dim(array, k * width, width, array.ndim - 1) for k in places],
                axis=-1,
            )

        def sequence(rows):
            other = swap(rows, "tp")
            return jnp.concatenate(
                [jnp.where(tp == 0, rows, other), jnp.where(tp == 0, other, rows)], axis=0
            )

        def both_sequences(rows):
            away = swap(rows, "rep")
            return sequence(rows), sequence(away)

        def chip_sum(partial):
            other = swap(half(partial, 0, 1 - tp), "tp")
            return half(partial, 0, tp).astype(jnp.float32) + other.astype(jnp.float32)

        def project_out(mine, theirs, blocks, group):
            sums = []
            for start in range(0, len(blocks), group):
                weight = jnp.concatenate(blocks[start : start + group], axis=1)
                outs = []
                for rows in (theirs, mine):
                    outs.append(
                        jnp.dot(rows, weight, preferred_element_type=jnp.float32).astype(
                            jnp.bfloat16
                        )
                    )
                away = swap(chip_sum(outs[0]).astype(jnp.bfloat16), "rep")
                sums.append(chip_sum(outs[1]) + away.astype(jnp.float32))
            return jnp.concatenate(sums, axis=1)

        w_in = jnp.concatenate([half(w, 1, rep) for w in (w_bgate, w_cgate, w_value)], axis=1)
        w_gu = jnp.concatenate([half(w, 1, rep) for w in (w_gate, w_up)], axis=1)
        in_blocks = ring_first(w_in)
        out_blocks = ring_first(half(w_mixout, 0, rep))
        upper, lower = jnp.split(w_gu, 2, axis=0)
        gu_blocks = [part for both in zip(pair_first(upper), ring_first(lower)) for part in both]
        down_blocks = ring_first(half(w_down, 0, rep))

        channels = w_in.shape[1] // 3
        taps = lax.dynamic_slice_in_dim(conv_taps, (tp * 2 + rep) * channels, channels, 1)
        local = arrival_order(tokens)

        def mix(normed, weight):
            projected = jnp.dot(normed, weight, preferred_element_type=jnp.float32).astype(
                jnp.bfloat16
            )
            b_proj, c_proj, u_proj = (
                projected[:, k * channels : (k + 1) * channels].astype(jnp.float32)
                for k in range(3)
            )
            return (b_proj * causal_taps(c_proj * u_proj, taps)).astype(jnp.bfloat16)

        mine, theirs = both_sequences(rms_scale(local, arrival_order(mix_gain)).astype(jnp.bfloat16))
        weight = jnp.concatenate(in_blocks, axis=0)
        theirs, mine = mix(theirs, weight), mix(mine, weight)
        mixed = project_out(mine, theirs, out_blocks, 2)
        residual = local.astype(jnp.float32) + mixed

        units = w_gu.shape[1] // 2

        def feed(normed, weight):
            both = jnp.dot(normed, weight, preferred_element_type=jnp.float32)
            return (jax.nn.silu(both[:, :units]) * both[:, units:]).astype(jnp.bfloat16)

        mine, theirs = both_sequences(rms_scale(residual, arrival_order(mlp_gain)).astype(jnp.bfloat16))
        weight = jnp.concatenate(gu_blocks, axis=0)
        theirs, mine = feed(theirs, weight), feed(mine, weight)
        down = project_out(mine, theirs, down_blocks, 2)
        return global_order((residual + 0.5 * down).astype(jnp.bfloat16))

    return on_device


MESH = pl.DeviceIdType.MESH
STRIP = 16
LANES = 128
INPUT, OUT, GU, DN = (0, 1, 2), (3,), (4,), (5,)


def f32(value):
    return value.astype(jnp.float32)


def mxu(left, right):
    return jnp.dot(left, right, preferred_element_type=jnp.float32)


def kernel(
    n_z,
    tok_hbm, gain_one, wb_hbm, wc_hbm, wu_hbm, taps, wo_hbm, gain_two, wgu_hbm, wd_hbm,
    out_hbm,
    wb, wc, wu, wo, wgu, wd,
    tok, normed, gated, part, theirs, outgo, income, res, normed_two, hidden,
    part_two, theirs_two, outgo_two, income_two, final,
    tail,
    load_sem, y_send, y_recv, zown_send, zfwd_send, z_recv, x_send, x_recv,
    one_send, one_recv, mix_send, mix_recv, mid_send, mid_recv, two_send, two_recv, store_sem,
):
    rep, fs, tp = (lax.axis_index(name) for name in ("rep", "fs", "tp"))
    z, y = lax.div(fs, 2), lax.rem(fs, 2)
    rows, _ = tok.shape
    sub = rows // 2
    depth = wb_hbm.shape[0]
    channels = wb.shape[1]
    pair_units = wgu.shape[1]
    units = pair_units // 2
    width = wo.shape[2]
    n_fs = 2 * n_z
    core = (rep, fs, 1 - tp)
    mate = (rep, z * 2 + 1 - y, tp)
    twin = (1 - rep, fs, tp)

    def along(position):
        return (rep, position * 2 + y, tp)

    def kth(k):
        near = jnp.minimum(z, n_z - 1 - z)
        both = z + ((k + 1) // 2) * (1 if k % 2 == 0 else -1)
        far = jnp.where(z < n_z - 1 - z, z + (k - near), z - (k - near))
        return jnp.where(k <= 2 * near, both, far)

    def line(rr, position):
        return position * 2 + (y if rr == 0 else 1 - y)

    def source(t, half, piece=None):
        parts = 2 if piece is None else 1
        first = 0 if piece is None else piece
        if t in OUT + DN:
            ref = (wo_hbm, wd_hbm)[t == 5]
            size = ref.shape[0] // 4
            return ref.at[pl.ds(pl.multiple_of((half * 2 + first) * size, 16), parts * size), :]
        ref = (wb_hbm, wc_hbm, wu_hbm, None, wgu_hbm)[t]
        cols = pair_units if t == 4 else channels
        size = depth // 2
        return ref.at[
            pl.ds(pl.multiple_of(first * size, 16), parts * size),
            pl.ds(pl.multiple_of(half * cols, 128), cols),
        ]

    def slot(t, index, piece=None):
        parts = 2 if piece is None else 1
        first = 0 if piece is None else piece
        if t in OUT + DN:
            ref = (wo, wd)[t == 5]
            size = ref.shape[1] // 2
            return ref.at[index, pl.ds(pl.multiple_of(first * size, 16), parts * size), :]
        ref = (wb, wc, wu, None, wgu)[t]
        size = depth // 2
        return ref.at[pl.ds(pl.multiple_of(index * depth + first * size, 16), parts * size), :]

    def remote(src, dst, send, recv, device):
        return pltpu.make_async_remote_copy(
            src_ref=src, dst_ref=dst, send_sem=send, recv_sem=recv, device_id=device, device_id_type=MESH
        )


    def local(t):
        return pltpu.make_async_copy(source(t, y), slot(t, fs), load_sem.at[t])

    def y_copy(t, index):
        return remote(source(t, 1 - y), slot(t, index), y_send.at[t], y_recv.at[t], mate)

    def z_own(t, rr, side):
        index = line(rr, z)
        src = source(t, y, rep) if rr == 0 else slot(t, index, rep)
        return remote(
            src, slot(t, index, rep), zown_send.at[t, rr, (side + 1) // 2], z_recv.at[t, rr, z], along(z + side)
        )

    def z_fwd(t, rr, position, target):
        place = slot(t, line(rr, position), rep)
        return remote(place, place, zfwd_send.at[t, rr, position], z_recv.at[t, rr, position], along(target))

    def x_copy(t, rr, position, piece):
        place = slot(t, line(rr, position), piece)
        return remote(place, place, x_send.at[t, rr, position], x_recv.at[t, rr, position], twin)

    def z_each(group, rr, act):
        for side in (-1, 1):

            @pl.when(jnp.logical_and(z + side >= 0, z + side < n_z))
            def _():
                for t in group:
                    act(z_own(t, rr, side))

    def start_own(group, rr):
        if rr == 1:
            for t in group:
                y_copy(t, line(1, z)).wait_recv()
        z_each(group, rr, lambda copy: copy.start())

    def relay(group, rr, k):
        position = kth(k)
        onward = z + jnp.where(position < z, 1, -1)
        for t in group:
            z_fwd(t, rr, position, z).wait_recv()

            @pl.when(jnp.logical_and(onward >= 0, onward < n_z))
            def _(t=t):
                z_fwd(t, rr, position, onward).start()

            x_copy(t, rr, position, rep).start()

    def x_wait(group, pairs):
        for rr, k in pairs:
            for t in group:
                x_copy(t, rr, kth(k), 1 - rep).wait_recv()

    everything = [(rr, k) for rr in range(2) for k in range(1, n_z)]


    def half_rows(which, first=0, count=None):
        return pl.ds(pl.multiple_of(which * rows + first, 16), rows if count is None else count)

    def core_copy(src, dst, sems, place):
        return remote(src, dst, sems[0].at[place], sems[1].at[place], core)

    def mate_copy(src, dst, sems, place):
        return remote(src, dst, sems[0].at[place], sems[1].at[place], mate)

    one, mix, mid, two = (one_send, one_recv), (mix_send, mix_recv), (mid_send, mid_recv), (two_send, two_recv)
    mine, other = half_rows(tp), half_rows(1 - tp)


    barrier = pltpu.get_barrier_semaphore()
    for device in (core, mate, twin):
        pl.semaphore_signal(barrier, inc=1, device_id=device, device_id_type=MESH)
    neighbours = 3
    for side in (-1, 1):
        inside = jnp.logical_and(z + side >= 0, z + side < n_z)
        neighbours += inside.astype(jnp.int32)

        @pl.when(inside)
        def _(side=side):
            pl.semaphore_signal(barrier, inc=1, device_id=along(z + side), device_id_type=MESH)

    load = pltpu.make_async_copy(tok_hbm, tok, load_sem.at[6])
    load.start()
    pl.semaphore_wait(barrier, neighbours)
    for t in INPUT:
        y_copy(t, fs).start()
        z_each((t,), 0, lambda copy: copy.start())
    for t in INPUT + OUT + GU + DN:
        local(t).start()
    load.wait()

    @pl.loop(0, rows // STRIP)
    def _(i):
        at = pl.ds(pl.multiple_of(i * STRIP, STRIP), STRIP)
        values = f32(tok[at, :])
        factor = lax.rsqrt(jnp.mean(values * values, axis=-1, keepdims=True) + 1e-06)
        normed[0, pl.ds(pl.multiple_of(tp * rows + i * STRIP, STRIP), STRIP), :] = (
            values * factor * gain_one[...]
        ).astype(jnp.bfloat16)

    one_core = core_copy(normed.at[0, mine, :], normed.at[0, mine, :], one, 0)
    one_mate = mate_copy(normed.at[0, mine, :], normed.at[1, mine, :], one, 1)
    one_pass = core_copy(normed.at[1, mine, :], normed.at[1, mine, :], one, 2)
    one_core.start()
    one_mate.start()
    for t in OUT + GU + DN:
        y_copy(t, fs).start()


    for k in range(1, n_z):
        relay(INPUT, 0, k)
    start_own(INPUT, 1)
    for k in range(1, n_z):
        relay(INPUT, 1, k)
    one_mate.wait_recv()
    one_pass.start()
    start_own(OUT, 0)
    start_own(OUT, 1)
    for t in INPUT:
        local(t).wait()
    x_wait(INPUT, everything)
    core_copy(normed.at[0, other, :], normed.at[0, other, :], one, 0).wait_recv()
    core_copy(normed.at[1, other, :], normed.at[1, other, :], one, 2).wait_recv()

    my_taps = pl.ds(pl.multiple_of((tp * 2 + y) * channels, 128), channels)

    def project_in(seq, half):
        at = pl.ds(half * rows, rows)
        part_rows = normed[seq, at, :]
        mixed = f32(mxu(part_rows, wc[...]).astype(jnp.bfloat16)) * f32(mxu(part_rows, wu[...]).astype(jnp.bfloat16))
        row = lax.broadcasted_iota(jnp.int32, mixed.shape, 0)
        before = [jnp.zeros((1, channels), jnp.float32)] * 2 if half == 0 else [tail[0:1, :], tail[1:2, :]]
        back_one = jnp.where(row == 0, before[1], pltpu.roll(mixed, 1, 0))
        back_two = jnp.where(row == 0, before[0], jnp.where(row == 1, before[1], pltpu.roll(mixed, 2, 0)))
        if half == 0:
            tail[0:2, :] = mixed[rows - 2 : rows, :]
        convolved = (
            taps[0:1, my_taps] * back_two + taps[1:2, my_taps] * back_one + taps[2:3, my_taps] * mixed
        )
        b_proj = f32(mxu(part_rows, wb[...]).astype(jnp.bfloat16))
        gated[seq, at, :] = (b_proj * convolved).astype(jnp.bfloat16)

    turns = list(everything)
    for seq in (1, 0):
        for half in range(2):
            project_in(seq, half)
            for rr, k in turns[:2]:
                relay(OUT, rr, k)
            turns = turns[2:]
    for rr, k in turns:
        relay(OUT, rr, k)
    start_own(GU, 0)
    start_own(GU, 1)
    local(3).wait()
    x_wait(OUT, everything)

    def project_out(seq, at):
        left = gated[seq, at, :]
        for index in range(n_fs):
            part[seq, at, index * width : (index + 1) * width] = mxu(left, wo[index]).astype(jnp.bfloat16)

    mix_core = [core_copy(part.at[s, other, :], theirs.at[s], mix, s) for s in range(2)]
    project_out(1, other)
    mix_core[1].start()
    project_out(1, mine)
    mix_core[1].wait_recv()
    halves = [pl.ds(i * sub, sub) for i in range(2)]
    mix_mate = [mate_copy(outgo.at[at, :], income.at[at, :], mix, 2 + i) for i, at in enumerate(halves)]
    strips = sub // STRIP
    for i in range(2):

        @pl.loop(0, strips)
        def _(j, i=i):
            first = i * sub + j * STRIP
            at = pl.ds(pl.multiple_of(first, STRIP), STRIP)
            outgo[at, :] = (f32(part[1, half_rows(tp, first, STRIP), :]) + f32(theirs[1, at, :])).astype(jnp.bfloat16)

        mix_mate[i].start()
    relay(GU, 0, 1)
    project_out(0, other)
    mix_core[0].start()
    project_out(0, mine)
    mix_core[0].wait_recv()
    relay(GU, 0, 2)
    relay(GU, 0, 3) if n_z > 3 else None

    def piece(which, i):
        return half_rows(which, i * sub, sub)

    def mid_core(which, i):
        return core_copy(normed_two.at[0, piece(which, i), :], normed_two.at[0, piece(which, i), :], mid, i)

    def mid_mate(i):
        return mate_copy(normed_two.at[0, piece(tp, i), :], normed_two.at[1, piece(tp, i), :], mid, 2 + i)

    def mid_pass(which, i):
        return core_copy(normed_two.at[1, piece(which, i), :], normed_two.at[1, piece(which, i), :], mid, 4 + i)

    for i in range(2):
        mix_mate[i].wait_recv()

        @pl.loop(0, strips)
        def _(j, i=i):
            first = i * sub + j * STRIP
            at = pl.ds(pl.multiple_of(first, STRIP), STRIP)
            here = half_rows(tp, first, STRIP)
            values = f32(tok[at, :]) + ((f32(part[0, here, :]) + f32(theirs[0, at, :])) + f32(income[at, :]))
            res[at, :] = values
            factor = lax.rsqrt(jnp.mean(values * values, axis=-1, keepdims=True) + 1e-06)
            normed_two[0, here, :] = (values * factor * gain_two[...]).astype(jnp.bfloat16)

        mid_mate(i).start()
        mid_core(tp, i).start()
        if i == 0:
            relay(GU, 1, 1)
    for k in range(2, n_z):
        relay(GU, 1, k)
    start_own(DN, 0)
    start_own(DN, 1)


    def feed(seq, at):
        both = mxu(normed_two[seq, at, :], wgu[...])
        gate, up = both[:, :units], both[:, units:]
        hidden[seq, at, :] = (gate / (1.0 + jnp.exp(-gate)) * up).astype(jnp.bfloat16)

    mid_mate(0).wait_recv()
    mid_pass(tp, 0).start()
    local(4).wait()
    x_wait(GU, everything)
    feed(0, mine)
    relay(DN, 0, 1)
    mid_core(1 - tp, 0).wait_recv()
    mid_core(1 - tp, 1).wait_recv()
    feed(0, other)
    relay(DN, 0, 2)
    feed(1, piece(tp, 0))
    mid_pass(1 - tp, 0).wait_recv()
    feed(1, piece(1 - tp, 0))
    for k in range(3, n_z):
        relay(DN, 0, k)
    mid_mate(1).wait_recv()
    mid_pass(tp, 1).start()
    relay(DN, 1, 1)
    feed(1, piece(tp, 1))
    mid_pass(1 - tp, 1).wait_recv()
    feed(1, piece(1 - tp, 1))
    local(5).wait()

    def two_core(index):
        return core_copy(part_two.at[index, :, other, :], theirs_two.at[index], two, index)

    def two_mate(index):
        return mate_copy(outgo_two.at[index], income_two.at[index], two, n_fs + index)

    def down(index):
        right = wd[index]
        for seq in range(2):
            for half in range(2):
                at = pl.ds(half * rows, rows)
                part_two[index, seq, at, :] = mxu(hidden[seq, at, :], right).astype(jnp.bfloat16)
        two_core(index).start()

    def add_cores(index):
        two_core(index).wait_recv()
        outgo_two[index] = (f32(part_two[index, 1, mine, :]) + f32(theirs_two[index, 1])).astype(jnp.bfloat16)
        two_mate(index).start()

    order = [line(rr, z if k == 0 else kth(k)) for k in range(n_z) for rr in range(2)]
    for place, index in enumerate(order):
        k, rr = place // 2, place % 2
        if k > 0:
            x_wait(DN, [(rr, k)])
        down(index)
        if place > 0:
            add_cores(order[place - 1])
        if 1 <= place < n_z - 1:
            relay(DN, 1, place + 1)
    add_cores(order[-1])
    stores = []
    for place, index in enumerate(order):
        two_mate(index).wait_recv()
        cols = pl.ds(pl.multiple_of(index * width, 128), width)
        total = (f32(part_two[index, 0, mine, :]) + f32(theirs_two[index, 0])) + f32(income_two[index])
        final[:, cols] = (res[:, cols] + 0.5 * total).astype(jnp.bfloat16)
        stores.append(pltpu.make_async_copy(final.at[:, cols], out_hbm.at[:, cols], store_sem.at[place]))
        stores[-1].start()


    for t in INPUT + OUT + GU + DN:
        y_copy(t, fs).wait_send()
        for rr in range(2):
            z_each((t,), rr, lambda copy: copy.wait_send())
            for k in range(1, n_z):
                position = kth(k)
                onward = z + jnp.where(position < z, 1, -1)
                x_copy(t, rr, position, rep).wait_send()

                @pl.when(jnp.logical_and(onward >= 0, onward < n_z))
                def _(t=t, rr=rr, position=position, onward=onward):
                    z_fwd(t, rr, position, onward).wait_send()

    sent = [one_core, one_mate, one_pass, *mix_core, *mix_mate]
    sent += [make for i in range(2) for make in (mid_core(tp, i), mid_mate(i), mid_pass(tp, i))]
    sent += [make for index in order for make in (two_core(index), two_mate(index))]
    for copy in sent:
        copy.wait_send()
    for copy in stores:
        copy.wait()


def block(
    n_fs, tokens, mix_gain, w_bgate, w_cgate, w_value, conv_taps, w_mixout, mlp_gain, w_gate, w_up, w_down
):
    rows, dim = tokens.shape
    depth, channels = w_bgate.shape[0], w_bgate.shape[1] // 2
    units = w_gate.shape[1] // 2
    width = w_mixout.shape[1]
    n_z = n_fs // 2
    bf16 = jnp.bfloat16
    w_gu = jnp.concatenate(
        [w[:, h * units : (h + 1) * units] for h in range(2) for w in (w_gate, w_up)], axis=1
    )
    hbm = pl.BlockSpec(memory_space=pl.ANY)
    vmem = pl.BlockSpec(memory_space=pltpu.VMEM)
    dma = pltpu.SemaphoreType.DMA
    return pl.pallas_call(
        functools.partial(kernel, n_z),
        out_shape=jax.ShapeDtypeStruct(tokens.shape, tokens.dtype),
        in_specs=[hbm, vmem, hbm, hbm, hbm, vmem, hbm, vmem, hbm, hbm],
        out_specs=hbm,
        scratch_shapes=[
            *[pltpu.VMEM((n_fs * depth, channels), bf16)] * 3,
            pltpu.VMEM((n_fs, w_mixout.shape[0] // 2, width), bf16),
            pltpu.VMEM((n_fs * depth, 2 * units), bf16),
            pltpu.VMEM((n_fs, w_down.shape[0] // 2, width), bf16),
            pltpu.VMEM((rows, dim), bf16),
            pltpu.VMEM((2, 2 * rows, dim), bf16),
            pltpu.VMEM((2, 2 * rows, channels), bf16),
            pltpu.VMEM((2, 2 * rows, dim), bf16),
            pltpu.VMEM((2, rows, dim), bf16),
            pltpu.VMEM((rows, dim), bf16),
            pltpu.VMEM((rows, dim), bf16),
            pltpu.VMEM((rows, dim), jnp.float32),
            pltpu.VMEM((2, 2 * rows, dim), bf16),
            pltpu.VMEM((2, 2 * rows, units), bf16),
            pltpu.VMEM((n_fs, 2, 2 * rows, width), bf16),
            pltpu.VMEM((n_fs, 2, rows, width), bf16),
            pltpu.VMEM((n_fs, rows, width), bf16),
            pltpu.VMEM((n_fs, rows, width), bf16),
            pltpu.VMEM((rows, dim), bf16),
            pltpu.VMEM((8, channels), jnp.float32),
            dma((7,)),
            dma((6,)),
            dma((6,)),
            dma((6, 2, 2)),
            *[dma((6, 2, n_z))] * 4,
            *[dma((3,))] * 2,
            *[dma((4,))] * 2,
            *[dma((6,))] * 2,
            *[dma((2 * n_fs,))] * 2,
            dma((n_fs,)),
        ],
        compiler_params=pltpu.CompilerParams(
            collective_id=0, has_side_effects=True, vmem_limit_bytes=66_900_000
        ),
    )(
        tokens, mix_gain[None], w_bgate, w_cgate, w_value, conv_taps, w_mixout, mlp_gain[None], w_gu, w_down
    )


SPECS = (
    P(("rep", "fs", "tp"), None),
    P(),
    P("fs", "tp"),
    P("fs", "tp"),
    P("fs", "tp"),
    P(),
    P("tp", "fs"),
    P(),
    P("fs", "tp"),
    P("fs", "tp"),
    P("tp", "fs"),
)


def permuted(mesh):
    return jax.shard_map(
        build(mesh.shape["fs"]),
        mesh=mesh,
        in_specs=SPECS,
        out_specs=P(("rep", "fs", "tp"), None),
        check_vma=False,
    )


def fused(mesh):
    return jax.shard_map(
        functools.partial(block, mesh.shape["fs"]),
        mesh=mesh,
        in_specs=SPECS,
        out_specs=P(("rep", "fs", "tp"), None),
        check_vma=False,
    )


def solution(mesh):
    n_fs, n_rep, n_tp = (mesh.shape[name] for name in ("fs", "rep", "tp"))

    def step(*operands):
        tokens, w_down = operands[0], operands[-1]
        rows = tokens.shape[0] // (n_rep * n_fs * n_tp)
        width = tokens.shape[1] // n_fs
        units = w_down.shape[0] // n_tp
        aligned = (
            (n_rep, n_tp, n_fs % 2) == (2, 2, 0)
            and (rows % (2 * STRIP), width % LANES, units % (4 * STRIP), units % LANES) == (0, 0, 0, 0)
            and tokens.shape[1] % (4 * LANES) == 0
        )
        return (fused if aligned else permuted)(mesh)(*operands)

    return step
```

```python
import functools

import jax
import jax.numpy as jnp
from jax import lax
from jax.experimental import pallas as pl
from jax.experimental.pallas import tpu as pltpu
from jax.sharding import PartitionSpec as P


def rms_scale(matrix, gain):
    values = matrix.astype(jnp.float32)
    factor = lax.rsqrt(jnp.mean(values * values, axis=-1, keepdims=True) + 1e-06)
    return values * factor * gain


def causal_taps(mixed, filters):
    length = mixed.shape[-2]
    padded = jnp.pad(mixed, [(2, 0), (0, 0)])
    return (
        filters[0] * padded[0:length]
        + filters[1] * padded[1 : length + 1]
        + filters[2] * padded[2 : length + 2]
    )


def swap(array, axis):
    return lax.ppermute(array, axis, [(0, 1), (1, 0)])


def half(array, axis, part):
    size = array.shape[axis] // 2
    return lax.dynamic_slice_in_dim(array, part * size, size, axis)


def build(n_fs):
    ring = [(i, (i + 2) % n_fs) for i in range(n_fs)]
    pair = [(i, i ^ 1) for i in range(n_fs)]
    steps = n_fs // 2

    def ring_first(block):
        blocks = []
        for step in range(steps):
            blocks += [block, lax.ppermute(block, "fs", pair)]
            if step < steps - 1:
                block = lax.ppermute(block, "fs", ring)
        return blocks

    def pair_first(block):
        mate = lax.ppermute(block, "fs", pair)
        blocks = []
        for step in range(steps):
            blocks += [block, mate]
            if step < steps - 1:
                block = lax.ppermute(block, "fs", ring)
                mate = lax.ppermute(mate, "fs", ring)
        return blocks

    def on_device(
        tokens, mix_gain, w_bgate, w_cgate, w_value, conv_taps, w_mixout, mlp_gain, w_gate, w_up, w_down
    ):
        rep, fs, tp = (lax.axis_index(name) for name in ("rep", "fs", "tp"))
        width = tokens.shape[1] // n_fs

        def arrival_order(array):
            order = [((fs ^ j) - 2 * s + n_fs) % n_fs for s in range(steps) for j in range(2)]
            return jnp.concatenate(
                [lax.dynamic_slice_in_dim(array, k * width, width, array.ndim - 1) for k in order],
                axis=-1,
            )

        def global_order(array):
            places = []
            for k in range(n_fs):
                j = (fs ^ k) & 1
                places.append((((fs ^ j) - k + n_fs) % n_fs) + j)
            return jnp.concatenate(
                [lax.dynamic_slice_in_dim(array, k * width, width, array.ndim - 1) for k in places],
                axis=-1,
            )

        def sequence(rows):
            other = swap(rows, "tp")
            return jnp.concatenate(
                [jnp.where(tp == 0, rows, other), jnp.where(tp == 0, other, rows)], axis=0
            )

        def both_sequences(rows):
            away = swap(rows, "rep")
            return sequence(rows), sequence(away)

        def chip_sum(partial):
            other = swap(half(partial, 0, 1 - tp), "tp")
            return half(partial, 0, tp).astype(jnp.float32) + other.astype(jnp.float32)

        def project_out(mine, theirs, blocks, group):
            sums = []
            for start in range(0, len(blocks), group):
                weight = jnp.concatenate(blocks[start : start + group], axis=1)
                outs = []
                for rows in (theirs, mine):
                    outs.append(
                        jnp.dot(rows, weight, preferred_element_type=jnp.float32).astype(
                            jnp.bfloat16
                        )
                    )
                away = swap(chip_sum(outs[0]).astype(jnp.bfloat16), "rep")
                sums.append(chip_sum(outs[1]) + away.astype(jnp.float32))
            return jnp.concatenate(sums, axis=1)

        w_in = jnp.concatenate([half(w, 1, rep) for w in (w_bgate, w_cgate, w_value)], axis=1)
        w_gu = jnp.concatenate([half(w, 1, rep) for w in (w_gate, w_up)], axis=1)
        in_blocks = ring_first(w_in)
        out_blocks = ring_first(half(w_mixout, 0, rep))
        upper, lower = jnp.split(w_gu, 2, axis=0)
        gu_blocks = [part for both in zip(pair_first(upper), ring_first(lower)) for part in both]
        down_blocks = ring_first(half(w_down, 0, rep))

        channels = w_in.shape[1] // 3
        taps = lax.dynamic_slice_in_dim(conv_taps, (tp * 2 + rep) * channels, channels, 1)
        local = arrival_order(tokens)

        def mix(normed, weight):
            projected = jnp.dot(normed, weight, preferred_element_type=jnp.float32).astype(
                jnp.bfloat16
            )
            b_proj, c_proj, u_proj = (
                projected[:, k * channels : (k + 1) * channels].astype(jnp.float32)
                for k in range(3)
            )
            return (b_proj * causal_taps(c_proj * u_proj, taps)).astype(jnp.bfloat16)

        mine, theirs = both_sequences(rms_scale(local, arrival_order(mix_gain)).astype(jnp.bfloat16))
        weight = jnp.concatenate(in_blocks, axis=0)
        theirs, mine = mix(theirs, weight), mix(mine, weight)
        mixed = project_out(mine, theirs, out_blocks, 2)
        residual = local.astype(jnp.float32) + mixed

        units = w_gu.shape[1] // 2

        def feed(normed, weight):
            both = jnp.dot(normed, weight, preferred_element_type=jnp.float32)
            return (jax.nn.silu(both[:, :units]) * both[:, units:]).astype(jnp.bfloat16)

        mine, theirs = both_sequences(rms_scale(residual, arrival_order(mlp_gain)).astype(jnp.bfloat16))
        weight = jnp.concatenate(gu_blocks, axis=0)
        theirs, mine = feed(theirs, weight), feed(mine, weight)
        down = project_out(mine, theirs, down_blocks, 2)
        return global_order((residual + 0.5 * down).astype(jnp.bfloat16))

    return on_device


MESH = pl.DeviceIdType.MESH
STRIP = 16
LANES = 128
C, U, B, OUT, GA, GB, DN = TYPES = range(7)
SHARED = (DN,)


def f32(value):
    return value.astype(jnp.float32)


def mxu(left, right):
    return jnp.dot(left, right, preferred_element_type=jnp.float32)


def kernel(
    n_z,
    tok_hbm, gain_one, wb_hbm, wc_hbm, wu_hbm, taps, wo_hbm, gain_two, wg_hbm, wup_hbm, wd_hbm,
    final,
    wb, wc, wu, wo, wgu, wd,
    raw_gate, raw_up, away,
    tok, normed, convolved, gated, part, theirs, outgo, income, res, normed_two, hidden,
    part_two, theirs_two, outgo_two, income_two,
    tail,
    load_sem, y_send, y_recv, zown_send, zfwd_send, z_recv, x_send, x_recv,
    one_send, one_recv, mix_send, mix_recv, mid_send, mid_recv, two_send, two_recv,
):
    rep, fs, tp = (lax.axis_index(name) for name in ("rep", "fs", "tp"))
    z, y = lax.div(fs, 2), lax.rem(fs, 2)
    rows, _ = tok.shape
    sub = rows // 2
    depth = wb_hbm.shape[0]
    channels = wb.shape[1]
    pair_units = wgu.shape[1]
    units = pair_units // 2
    width = wo.shape[2]
    n_fs = 2 * n_z
    core = (rep, fs, 1 - tp)
    mate = (rep, z * 2 + 1 - y, tp)
    twin = (1 - rep, fs, tp)

    def along(position):
        return (rep, position * 2 + y, tp)

    def kth(k):
        near = jnp.minimum(z, n_z - 1 - z)
        longer = jnp.where(z < n_z - 1 - z, 1, -1)
        both = z + longer * (((k + 1) // 2) * (1 if k % 2 == 1 else -1))
        return jnp.where(k <= 2 * near, both, z + longer * (k - near))

    def line(rr, position):
        return position * 2 + (y if rr == 0 else 1 - y)

    def rows_of(t, piece, base):
        if t in (OUT, DN):
            size = (wo, wd)[t == DN].shape[1] // 2
        else:
            size = depth // (4 if t in (GA, GB) else 2)
        first = base + (2 * size if t == GB else 0)
        if piece is None:
            return pl.ds(pl.multiple_of(first, 16), 2 * size)
        return pl.ds(pl.multiple_of(first + piece * size, 16), size)

    def source(t, half, piece=None):
        if t in (OUT, DN):
            ref = (wo_hbm, wd_hbm)[t == DN]
            return ref.at[rows_of(t, piece, half * (ref.shape[0] // 2)), :]
        ref = (wc_hbm, wu_hbm, wb_hbm)[t]
        return ref.at[rows_of(t, piece, 0), pl.ds(pl.multiple_of(half * channels, 128), channels)]

    def slot(t, index, piece=None):
        if t in (OUT, DN):
            return (wo, wd)[t == DN].at[index, rows_of(t, piece, 0), :]
        return (wc, wu, wb, None, wgu, wgu)[t].at[rows_of(t, piece, index * depth), :]

    def remote(src, dst, send, recv, device):
        return pltpu.make_async_remote_copy(
            src_ref=src, dst_ref=dst, send_sem=send, recv_sem=recv, device_id=device, device_id_type=MESH
        )


    def local(t):
        return pltpu.make_async_copy(source(t, y), slot(t, fs), load_sem.at[t])

    def y_copy(t, index):
        piece = rep if t in SHARED else None
        src = away.at[rows_of(t, piece, 0), :] if t in (GA, GB) else source(t, 1 - y, piece)
        return remote(src, slot(t, index, piece), y_send.at[t], y_recv.at[t], mate)

    def z_own(t, rr, side):
        index = line(rr, z)
        src = slot(t, index, rep) if rr == 1 or t in (GA, GB) else source(t, y, rep)
        return remote(
            src, slot(t, index, rep), zown_send.at[t, rr, (side + 1) // 2], z_recv.at[t, rr, z], along(z + side)
        )

    def z_fwd(t, rr, position, target):
        place = slot(t, line(rr, position), rep)
        return remote(place, place, zfwd_send.at[t, rr, position], z_recv.at[t, rr, position], along(target))

    def x_copy(t, rr, position, piece):
        place = slot(t, line(rr, position), piece)
        return remote(place, place, x_send.at[t, rr, position], x_recv.at[t, rr, position], twin)

    def z_each(t, rr, act):
        for side in (-1, 1):

            @pl.when(jnp.logical_and(z + side >= 0, z + side < n_z))
            def _():
                act(z_own(t, rr, side))

    def start_own(t, rr):
        if rr == 1:
            y_copy(t, line(1, z)).wait_recv()
            if t in SHARED:
                x_copy(t, 1, z, rep).start()
        z_each(t, rr, lambda copy: copy.start())

    def relay(t, rr, k):
        position = kth(k)
        onward = z + jnp.where(position < z, 1, -1)
        z_fwd(t, rr, position, z).wait_recv()

        @pl.when(jnp.logical_and(onward >= 0, onward < n_z))
        def _():
            z_fwd(t, rr, position, onward).start()

        x_copy(t, rr, position, rep).start()

    def x_wait(t, pairs):
        for rr, k in pairs:
            x_copy(t, rr, kth(k), 1 - rep).wait_recv()

    def x_all(t):
        x_wait(t, [(rr, k) for rr in range(2) for k in range(1, n_z)] + [(1, 0)] * (t in SHARED))


    def half_rows(which, first=0, count=None):
        return pl.ds(pl.multiple_of(which * rows + first, 16), rows if count is None else count)

    def core_copy(src, dst, sems, place):
        return remote(src, dst, sems[0].at[place], sems[1].at[place], core)

    def mate_copy(src, dst, sems, place):
        return remote(src, dst, sems[0].at[place], sems[1].at[place], mate)

    one, mix, mid, two = (one_send, one_recv), (mix_send, mix_recv), (mid_send, mid_recv), (two_send, two_recv)
    mine, other = half_rows(tp), half_rows(1 - tp)


    barrier = pltpu.get_barrier_semaphore()
    for device in (core, mate, twin):
        pl.semaphore_signal(barrier, inc=1, device_id=device, device_id_type=MESH)
    neighbours = 3
    for side in (-1, 1):
        inside = jnp.logical_and(z + side >= 0, z + side < n_z)
        neighbours += inside.astype(jnp.int32)

        @pl.when(inside)
        def _(side=side):
            pl.semaphore_signal(barrier, inc=1, device_id=along(z + side), device_id_type=MESH)

    raw = [
        pltpu.make_async_copy(src, dst, load_sem.at[place])
        for src, dst, place in ((tok_hbm, tok, GA), (wg_hbm, raw_gate, GB), (wup_hbm, raw_up, DN + 1))
    ]
    raw[0].start()
    pl.semaphore_wait(barrier, neighbours)
    for t in (C, U, B):
        y_copy(t, fs).start()
    for t in (C, U, B):
        start_own(t, 0)
    for copy in raw[1:]:
        copy.start()
    for t in (C, U, B, OUT, DN):
        local(t).start()
    raw[0].wait()

    @pl.loop(0, rows // STRIP)
    def _(i):
        at = pl.ds(pl.multiple_of(i * STRIP, STRIP), STRIP)
        values = f32(tok[at, :])
        factor = lax.rsqrt(jnp.mean(values * values, axis=-1, keepdims=True) + 1e-06)
        normed[0, pl.ds(pl.multiple_of(tp * rows + i * STRIP, STRIP), STRIP), :] = (
            values * factor * gain_one[...]
        ).astype(jnp.bfloat16)

    one_core = core_copy(normed.at[0, mine, :], normed.at[0, mine, :], one, 0)
    one_mate = mate_copy(normed.at[0, mine, :], normed.at[1, mine, :], one, 1)
    one_pass = core_copy(normed.at[1, mine, :], normed.at[1, mine, :], one, 2)
    y_copy(OUT, fs).start()
    one_core.start()
    one_mate.start()

    def relays(types, rr, k):
        for t in types:
            relay(t, rr, k)

    three = (C, U, B)
    relays(three, 0, 1)
    start_own(C, 1)
    for copy in raw[1:]:
        copy.wait()

    @pl.loop(0, depth // STRIP)
    def _(i):
        at = pl.ds(pl.multiple_of(i * STRIP, STRIP), STRIP)
        here = pl.ds(pl.multiple_of(fs * depth + i * STRIP, STRIP), STRIP)
        gate, up = f32(raw_gate[at, :]), f32(raw_up[at, :])
        for half in range(2):
            cut = slice(half * units, (half + 1) * units)
            both = jnp.concatenate([gate[:, cut], up[:, cut]], axis=1).astype(jnp.bfloat16)

            @pl.when(y == half)
            def _(both=both):
                wgu[here, :] = both

            @pl.when(y != half)
            def _(both=both):
                away[at, :] = both

    for t in (GA, GB, DN):
        y_copy(t, fs).start()


    my_taps = pl.ds(pl.multiple_of((tp * 2 + y) * channels, 128), channels)

    def convolve(seq, half):
        at = pl.ds(half * rows, rows)
        left = normed[seq, at, :]
        mixed = f32(mxu(left, wc[...]).astype(jnp.bfloat16)) * f32(mxu(left, wu[...]).astype(jnp.bfloat16))
        row = lax.broadcasted_iota(jnp.int32, mixed.shape, 0)
        before = [jnp.zeros((1, channels), jnp.float32)] * 2 if half == 0 else [tail[0:1, :], tail[1:2, :]]
        back_one = jnp.where(row == 0, before[1], pltpu.roll(mixed, 1, 0))
        back_two = jnp.where(row == 0, before[0], jnp.where(row == 1, before[1], pltpu.roll(mixed, 2, 0)))
        if half == 0:
            tail[0:2, :] = mixed[rows - 2 : rows, :]
        convolved[seq, at, :] = (
            taps[0:1, my_taps] * back_two + taps[1:2, my_taps] * back_one + taps[2:3, my_taps] * mixed
        )

    def gate_out(seq, half):
        at = pl.ds(half * rows, rows)
        b_proj = f32(mxu(normed[seq, at, :], wb[...]).astype(jnp.bfloat16))
        gated[seq, at, :] = (b_proj * convolved[seq, at, :]).astype(jnp.bfloat16)

    arrivals = sorted((max(k, 2), rr, k) for rr in range(2) for k in range(1, n_z))
    for place, (_, rr, k) in enumerate(arrivals[1:]):
        if place == len(arrivals) - 3:
            start_own(OUT, 0)
        relays(three, rr, k)
        if place == 0:
            start_own(U, 1)
            start_own(B, 1)
    start_own(OUT, 1)
    relay(OUT, 0, 1)
    relay(OUT, 1, 1)
    one_mate.wait_recv()
    one_pass.start()
    for t in (C, U):
        local(t).wait()
        x_all(t)
    core_copy(normed.at[1, other, :], normed.at[1, other, :], one, 2).wait_recv()

    def mix_core(index):
        return core_copy(part.at[index, 1, other, :], theirs.at[index, 1], mix, index * 3)

    def mix_mate(index):
        return mate_copy(outgo.at[index], income.at[index], mix, index * 3 + 1)

    def mix_own(index):
        return core_copy(part.at[index, 0, other, :], theirs.at[index, 0], mix, index * 3 + 2)

    def project_out(index, seq):
        right = wo[index]
        for at in (other, mine):
            part[index, seq, at, :] = mxu(gated[seq, at, :], right).astype(jnp.bfloat16)
            if at is other:
                (mix_own, mix_core)[seq](index).start()

    def send_sum(index):
        mix_core(index).wait_recv()
        outgo[index] = (f32(part[index, 1, mine, :]) + f32(theirs[index, 1])).astype(jnp.bfloat16)
        mix_mate(index).start()

    order = [line(rr, kth(k)) for k in range(n_z) for rr in range(2)]

    convolve(1, 0)
    relay(OUT, 0, 2)
    convolve(1, 1)
    relay(OUT, 1, 2)
    local(B).wait()
    x_all(B)
    gate_out(1, 0)
    gate_out(1, 1)
    local(OUT).wait()
    project_out(order[0], 1)
    project_out(order[1], 1)
    send_sum(order[0])
    send_sum(order[1])
    for k in range(3, n_z):
        relay(OUT, 0, k)
        relay(OUT, 1, k)
    for t in (GA, GB):
        for rr in range(2):
            start_own(t, rr)
    core_copy(normed.at[0, other, :], normed.at[0, other, :], one, 0).wait_recv()
    gu = [(t, rr) for t in (GA, GB) for rr in range(2)]
    todo = [(*pair, k) for k in range(1, n_z) for pair in gu]
    todo.reverse()
    for place in range(2, 2 * n_z):
        x_wait(OUT, [(place % 2, place // 2)])
        project_out(order[place], 1)
        if place > 2:
            send_sum(order[place - 1])
        if place % 2 == 1:
            relay(*todo.pop())
    send_sum(order[-1])
    convolve(0, 0)
    relay(*todo.pop())
    convolve(0, 1)
    gate_out(0, 0)
    gate_out(0, 1)
    relay(*todo.pop())
    for index in order:
        project_out(index, 0)

    def add_up(index):
        mix_own(index).wait_recv()
        mix_mate(index).wait_recv()
        cols = pl.ds(pl.multiple_of(index * width, 128), width)
        res[:, cols] = f32(tok[:, cols]) + (
            (f32(part[index, 0, mine, :]) + f32(theirs[index, 0])) + f32(income[index])
        )

    relay(*todo.pop())
    relay(*todo.pop())
    for index in order:
        add_up(index)

    halves = [pl.ds(i * sub, sub) for i in range(2)]
    strips = sub // STRIP

    def piece(which, i):
        return half_rows(which, i * sub, sub)

    def mid_core(which, i):
        return core_copy(normed_two.at[0, piece(which, i), :], normed_two.at[0, piece(which, i), :], mid, i)

    def mid_mate(i):
        return mate_copy(normed_two.at[0, piece(tp, i), :], normed_two.at[1, piece(tp, i), :], mid, 2 + i)

    def mid_pass(which, i):
        return core_copy(normed_two.at[1, piece(which, i), :], normed_two.at[1, piece(which, i), :], mid, 4 + i)

    for i in range(2):

        @pl.loop(0, strips)
        def _(j, i=i):
            first = i * sub + j * STRIP
            at = pl.ds(pl.multiple_of(first, STRIP), STRIP)
            values = res[at, :]
            factor = lax.rsqrt(jnp.mean(values * values, axis=-1, keepdims=True) + 1e-06)
            normed_two[0, half_rows(tp, first, STRIP), :] = (values * factor * gain_two[...]).astype(jnp.bfloat16)

        mid_mate(i).start()
        mid_core(tp, i).start()
    while todo:
        relay(*todo.pop())
    start_own(DN, 0)
    start_own(DN, 1)


    def feed(seq, at):
        both = mxu(normed_two[seq, at, :], wgu[...])
        gate, up = both[:, :units], both[:, units:]
        hidden[seq, at, :] = (gate / (1.0 + jnp.exp(-gate)) * up).astype(jnp.bfloat16)

    def two_core(index, i):
        return core_copy(
            part_two.at[index, 1, piece(1 - tp, i), :], theirs_two.at[index, 1, halves[i], :], two, index * 5 + i
        )

    def two_mate(index, i):
        return mate_copy(
            outgo_two.at[index, halves[i], :], income_two.at[index, halves[i], :], two, index * 5 + 2 + i
        )

    def two_own(index):
        return core_copy(part_two.at[index, 0, other, :], theirs_two.at[index, 0], two, index * 5 + 4)

    def down(index, i):
        right = wd[index]
        for which in (1 - tp, tp):
            at = piece(which, i)
            part_two[index, 1, at, :] = mxu(hidden[1, at, :], right).astype(jnp.bfloat16)
        two_core(index, i).start()

    def add_cores(index, i):
        two_core(index, i).wait_recv()
        outgo_two[index, halves[i], :] = (
            f32(part_two[index, 1, piece(tp, i), :]) + f32(theirs_two[index, 1, halves[i], :])
        ).astype(jnp.bfloat16)
        two_mate(index, i).start()

    def down_own(index):
        right = wd[index]
        for at in (other, mine):
            part_two[index, 0, at, :] = mxu(hidden[0, at, :], right).astype(jnp.bfloat16)
        two_own(index).start()

    behind = []

    def step(place, i):
        down(order[place], i)
        if behind:
            add_cores(*behind.pop())
        behind.append((order[place], i))

    def flush():
        while behind:
            add_cores(*behind.pop())

    late = sorted((k, rr) for rr in range(2) for k in range(1, n_z))
    late.reverse()

    def relay_down():
        if late:
            k, rr = late.pop()
            relay(DN, rr, k)

    mid_mate(0).wait_recv()
    mid_pass(tp, 0).start()
    x_all(GA)
    x_all(GB)
    relay_down()
    feed(1, piece(tp, 0))
    relay_down()
    mid_pass(1 - tp, 0).wait_recv()
    feed(1, piece(1 - tp, 0))
    local(DN).wait()
    if DN in SHARED:
        x_wait(DN, [(1, 0)])
    step(0, 0)
    step(1, 0)
    flush()
    relay_down()
    mid_mate(1).wait_recv()
    mid_pass(tp, 1).start()
    feed(1, piece(tp, 1))
    mid_pass(1 - tp, 1).wait_recv()
    feed(1, piece(1 - tp, 1))
    step(0, 1)
    step(1, 1)
    flush()
    relay_down()
    for place in (2, 3):
        x_wait(DN, [(place % 2, place // 2)])
        step(place, 0)
        step(place, 1)
    flush()
    feed(0, mine)
    relay_down()
    mid_core(1 - tp, 0).wait_recv()
    mid_core(1 - tp, 1).wait_recv()
    feed(0, other)
    while late:
        relay_down()
    for place in range(4, n_fs):
        x_wait(DN, [(place % 2, place // 2)])
        for i in range(2):
            step(place, i)
        flush()
        down_own(order[place - 4])
    for place in range(n_fs - 4, n_fs):
        down_own(order[place])
    for index in order:
        two_own(index).wait_recv()
        for i in range(2):
            two_mate(index, i).wait_recv()
        cols = pl.ds(pl.multiple_of(index * width, 128), width)
        total = (f32(part_two[index, 0, mine, :]) + f32(theirs_two[index, 0])) + f32(income_two[index])
        final[:, cols] = (res[:, cols] + 0.5 * total).astype(jnp.bfloat16)


    for t in TYPES:
        y_copy(t, fs).wait_send()
        for rr in range(2):
            z_each(t, rr, lambda copy: copy.wait_send())
            for k in range(1, n_z):
                position = kth(k)
                onward = z + jnp.where(position < z, 1, -1)
                x_copy(t, rr, position, rep).wait_send()

                @pl.when(jnp.logical_and(onward >= 0, onward < n_z))
                def _(t=t, rr=rr, position=position, onward=onward):
                    z_fwd(t, rr, position, onward).wait_send()

            if rr == 1 and t in SHARED:
                x_copy(t, 1, z, rep).wait_send()
    sent = [one_core, one_mate, one_pass]
    sent += [make for i in range(2) for make in (mid_core(tp, i), mid_mate(i), mid_pass(tp, i))]
    for index in order:
        sent += [two_own(index), mix_core(index), mix_mate(index), mix_own(index)] + [make(index, i) for i in range(2) for make in (two_core, two_mate)]
    for copy in sent:
        copy.wait_send()


def block(
    n_fs, tokens, mix_gain, w_bgate, w_cgate, w_value, conv_taps, w_mixout, mlp_gain, w_gate, w_up, w_down
):
    rows, dim = tokens.shape
    depth, channels = w_bgate.shape[0], w_bgate.shape[1] // 2
    units = w_gate.shape[1] // 2
    width = w_mixout.shape[1]
    n_z = n_fs // 2
    bf16 = jnp.bfloat16
    hbm = pl.BlockSpec(memory_space=pl.ANY)
    vmem = pl.BlockSpec(memory_space=pltpu.VMEM)
    dma = pltpu.SemaphoreType.DMA
    return pl.pallas_call(
        functools.partial(kernel, n_z),
        out_shape=pltpu.VMEM(tokens.shape, tokens.dtype),
        in_specs=[hbm, vmem, hbm, hbm, hbm, vmem, hbm, vmem, hbm, hbm, hbm],
        out_specs=vmem,
        scratch_shapes=[
            *[pltpu.VMEM((n_fs * depth, channels), bf16)] * 3,
            pltpu.VMEM((n_fs, w_mixout.shape[0] // 2, width), bf16),
            pltpu.VMEM((n_fs * depth, 2 * units), bf16),
            pltpu.VMEM((n_fs, w_down.shape[0] // 2, width), bf16),
            *[pltpu.VMEM((depth, 2 * units), bf16)] * 3,
            pltpu.VMEM((rows, dim), bf16),
            pltpu.VMEM((2, 2 * rows, dim), bf16),
            pltpu.VMEM((2, 2 * rows, channels), jnp.float32),
            pltpu.VMEM((2, 2 * rows, channels), bf16),
            pltpu.VMEM((n_fs, 2, 2 * rows, width), bf16),
            pltpu.VMEM((n_fs, 2, rows, width), bf16),
            pltpu.VMEM((n_fs, rows, width), bf16),
            pltpu.VMEM((n_fs, rows, width), bf16),
            pltpu.VMEM((rows, dim), jnp.float32),
            pltpu.VMEM((2, 2 * rows, dim), bf16),
            pltpu.VMEM((2, 2 * rows, units), bf16),
            pltpu.VMEM((n_fs, 2, 2 * rows, width), bf16),
            pltpu.VMEM((n_fs, 2, rows, width), bf16),
            pltpu.VMEM((n_fs, rows, width), bf16),
            pltpu.VMEM((n_fs, rows, width), bf16),
            pltpu.VMEM((8, channels), jnp.float32),
            dma((8,)),
            *[dma((7,))] * 2,
            dma((7, 2, 2)),
            *[dma((7, 2, n_z))] * 4,
            *[dma((3,))] * 2,
            *[dma((3 * n_fs,))] * 2,
            *[dma((6,))] * 2,
            *[dma((5 * n_fs,))] * 2,
        ],
        compiler_params=pltpu.CompilerParams(
            collective_id=0, has_side_effects=True, vmem_limit_bytes=64_500_000
        ),
    )(
        tokens, mix_gain[None], w_bgate, w_cgate, w_value, conv_taps, w_mixout, mlp_gain[None], w_gate, w_up, w_down
    )


SPECS = (
    P(("rep", "fs", "tp"), None),
    P(),
    P("fs", "tp"),
    P("fs", "tp"),
    P("fs", "tp"),
    P(),
    P("tp", "fs"),
    P(),
    P("fs", "tp"),
    P("fs", "tp"),
    P("tp", "fs"),
)


def permuted(mesh):
    return jax.shard_map(
        build(mesh.shape["fs"]),
        mesh=mesh,
        in_specs=SPECS,
        out_specs=P(("rep", "fs", "tp"), None),
        check_vma=False,
    )


def fused(mesh):
    return jax.shard_map(
        functools.partial(block, mesh.shape["fs"]),
        mesh=mesh,
        in_specs=SPECS,
        out_specs=P(("rep", "fs", "tp"), None),
        check_vma=False,
    )


def solution(mesh):
    n_fs, n_rep, n_tp = (mesh.shape[name] for name in ("fs", "rep", "tp"))

    def step(*operands):
        tokens, w_down = operands[0], operands[-1]
        rows = tokens.shape[0] // (n_rep * n_fs * n_tp)
        width = tokens.shape[1] // n_fs
        units = w_down.shape[0] // n_tp
        aligned = (
            (n_rep, n_tp, n_fs % 2) == (2, 2, 0)
            and (rows % (2 * STRIP), width % LANES, units % (4 * STRIP), units % LANES) == (0, 0, 0, 0)
            and tokens.shape[1] % (4 * LANES) == 0
        )
        return (fused if aligned else permuted)(mesh)(*operands)

    return step
```

```python
import functools

import jax
import jax.numpy as jnp
from jax import lax
from jax.experimental import pallas as pl
from jax.experimental.pallas import tpu as pltpu
from jax.sharding import PartitionSpec as P


def rms_scale(matrix, gain):
    values = matrix.astype(jnp.float32)
    factor = lax.rsqrt(jnp.mean(values * values, axis=-1, keepdims=True) + 1e-06)
    return values * factor * gain


def causal_taps(mixed, filters):
    length = mixed.shape[-2]
    padded = jnp.pad(mixed, [(2, 0), (0, 0)])
    return (
        filters[0] * padded[0:length]
        + filters[1] * padded[1 : length + 1]
        + filters[2] * padded[2 : length + 2]
    )


def swap(array, axis):
    return lax.ppermute(array, axis, [(0, 1), (1, 0)])


def half(array, axis, part):
    size = array.shape[axis] // 2
    return lax.dynamic_slice_in_dim(array, part * size, size, axis)


def build(n_fs):
    ring = [(i, (i + 2) % n_fs) for i in range(n_fs)]
    pair = [(i, i ^ 1) for i in range(n_fs)]
    steps = n_fs // 2

    def ring_first(block):
        blocks = []
        for step in range(steps):
            blocks += [block, lax.ppermute(block, "fs", pair)]
            if step < steps - 1:
                block = lax.ppermute(block, "fs", ring)
        return blocks

    def pair_first(block):
        mate = lax.ppermute(block, "fs", pair)
        blocks = []
        for step in range(steps):
            blocks += [block, mate]
            if step < steps - 1:
                block = lax.ppermute(block, "fs", ring)
                mate = lax.ppermute(mate, "fs", ring)
        return blocks

    def on_device(
        tokens, mix_gain, w_bgate, w_cgate, w_value, conv_taps, w_mixout, mlp_gain, w_gate, w_up, w_down
    ):
        rep, fs, tp = (lax.axis_index(name) for name in ("rep", "fs", "tp"))
        width = tokens.shape[1] // n_fs

        def arrival_order(array):
            order = [((fs ^ j) - 2 * s + n_fs) % n_fs for s in range(steps) for j in range(2)]
            return jnp.concatenate(
                [lax.dynamic_slice_in_dim(array, k * width, width, array.ndim - 1) for k in order],
                axis=-1,
            )

        def global_order(array):
            places = []
            for k in range(n_fs):
                j = (fs ^ k) & 1
                places.append((((fs ^ j) - k + n_fs) % n_fs) + j)
            return jnp.concatenate(
                [lax.dynamic_slice_in_dim(array, k * width, width, array.ndim - 1) for k in places],
                axis=-1,
            )

        def sequence(rows):
            other = swap(rows, "tp")
            return jnp.concatenate(
                [jnp.where(tp == 0, rows, other), jnp.where(tp == 0, other, rows)], axis=0
            )

        def both_sequences(rows):
            away = swap(rows, "rep")
            return sequence(rows), sequence(away)

        def chip_sum(partial):
            other = swap(half(partial, 0, 1 - tp), "tp")
            return half(partial, 0, tp).astype(jnp.float32) + other.astype(jnp.float32)

        def project_out(mine, theirs, blocks, group):
            sums = []
            for start in range(0, len(blocks), group):
                weight = jnp.concatenate(blocks[start : start + group], axis=1)
                outs = []
                for rows in (theirs, mine):
                    outs.append(
                        jnp.dot(rows, weight, preferred_element_type=jnp.float32).astype(
                            jnp.bfloat16
                        )
                    )
                away = swap(chip_sum(outs[0]).astype(jnp.bfloat16), "rep")
                sums.append(chip_sum(outs[1]) + away.astype(jnp.float32))
            return jnp.concatenate(sums, axis=1)

        w_in = jnp.concatenate([half(w, 1, rep) for w in (w_bgate, w_cgate, w_value)], axis=1)
        w_gu = jnp.concatenate([half(w, 1, rep) for w in (w_gate, w_up)], axis=1)
        in_blocks = ring_first(w_in)
        out_blocks = ring_first(half(w_mixout, 0, rep))
        upper, lower = jnp.split(w_gu, 2, axis=0)
        gu_blocks = [part for both in zip(pair_first(upper), ring_first(lower)) for part in both]
        down_blocks = ring_first(half(w_down, 0, rep))

        channels = w_in.shape[1] // 3
        taps = lax.dynamic_slice_in_dim(conv_taps, (tp * 2 + rep) * channels, channels, 1)
        local = arrival_order(tokens)

        def mix(normed, weight):
            projected = jnp.dot(normed, weight, preferred_element_type=jnp.float32).astype(
                jnp.bfloat16
            )
            b_proj, c_proj, u_proj = (
                projected[:, k * channels : (k + 1) * channels].astype(jnp.float32)
                for k in range(3)
            )
            return (b_proj * causal_taps(c_proj * u_proj, taps)).astype(jnp.bfloat16)

        mine, theirs = both_sequences(rms_scale(local, arrival_order(mix_gain)).astype(jnp.bfloat16))
        weight = jnp.concatenate(in_blocks, axis=0)
        theirs, mine = mix(theirs, weight), mix(mine, weight)
        mixed = project_out(mine, theirs, out_blocks, 2)
        residual = local.astype(jnp.float32) + mixed

        units = w_gu.shape[1] // 2

        def feed(normed, weight):
            both = jnp.dot(normed, weight, preferred_element_type=jnp.float32)
            return (jax.nn.silu(both[:, :units]) * both[:, units:]).astype(jnp.bfloat16)

        mine, theirs = both_sequences(rms_scale(residual, arrival_order(mlp_gain)).astype(jnp.bfloat16))
        weight = jnp.concatenate(gu_blocks, axis=0)
        theirs, mine = feed(theirs, weight), feed(mine, weight)
        down = project_out(mine, theirs, down_blocks, 2)
        return global_order((residual + 0.5 * down).astype(jnp.bfloat16))

    return on_device


MESH = pl.DeviceIdType.MESH
STRIP = 16
LANES = 128
C, U, B, OUT, *GU, DN = TYPES = range(7)
SHARED = (DN,)


def f32(value):
    return value.astype(jnp.float32)


def mxu(left, right):
    return jnp.dot(left, right, preferred_element_type=jnp.float32)


def kernel(
    n_z,
    tok_hbm, gain_one, wb_hbm, wc_hbm, wu_hbm, taps, wo_hbm, gain_two, wg_hbm, wup_hbm, wd_hbm,
    final,
    wb, wc, wu, wo, wgu, wd,
    raw_gate, raw_up, away,
    tok, normed, convolved, gated, part, theirs, outgo, income, res, normed_two, hidden,
    part_two, theirs_two, outgo_two, income_two,
    tail,
    load_sem, y_send, y_recv, z_send, z_recv, x_send, x_recv, x_each,
    one_send, one_recv, mix_send, mix_recv, mid_send, mid_recv, two_send, two_recv,
):
    rep, fs, tp = (lax.axis_index(name) for name in ("rep", "fs", "tp"))
    z, y = lax.div(fs, 2), lax.rem(fs, 2)
    rows, _ = tok.shape
    sub = rows // 2
    depth = wb_hbm.shape[0]
    channels = wb.shape[1]
    pair_units = wgu.shape[1]
    units = pair_units // 2
    width = wo.shape[2]
    n_fs = 2 * n_z
    core = (rep, fs, 1 - tp)
    mate = (rep, z * 2 + 1 - y, tp)
    twin = (1 - rep, fs, tp)

    def along(position):
        return (rep, position * 2 + y, tp)

    def kth(k):
        near = jnp.minimum(z, n_z - 1 - z)
        longer = jnp.where(z < n_z - 1 - z, 1, -1)
        both = z + longer * (((k + 1) // 2) * (1 if k % 2 == 1 else -1))
        return jnp.where(k <= 2 * near, both, z + longer * (k - near))

    def line(rr, position):
        return position * 2 + (y if rr == 0 else 1 - y)

    def rows_of(t, piece, base):
        if t in (OUT, DN):
            size = (wo, wd)[t == DN].shape[1] // 2
        else:
            size = depth // (2 * len(GU) if t in GU else 2)
        first = base + (2 * size * GU.index(t) if t in GU else 0)
        if piece is None:
            return pl.ds(pl.multiple_of(first, 16), 2 * size)
        return pl.ds(pl.multiple_of(first + piece * size, 16), size)

    def source(t, half, piece=None):
        if t in (OUT, DN):
            ref = (wo_hbm, wd_hbm)[t == DN]
            return ref.at[rows_of(t, piece, half * (ref.shape[0] // 2)), :]
        ref = (wc_hbm, wu_hbm, wb_hbm)[t]
        return ref.at[rows_of(t, piece, 0), pl.ds(pl.multiple_of(half * channels, 128), channels)]

    def slot(t, index, piece=None):
        if t in (OUT, DN):
            return (wo, wd)[t == DN].at[index, rows_of(t, piece, 0), :]
        return (wgu if t in GU else (wc, wu, wb)[t]).at[rows_of(t, piece, index * depth), :]

    def remote(src, dst, send, recv, device):
        return pltpu.make_async_remote_copy(
            src_ref=src, dst_ref=dst, send_sem=send, recv_sem=recv, device_id=device, device_id_type=MESH
        )


    def local(t):
        return pltpu.make_async_copy(source(t, y), slot(t, fs), load_sem.at[t])

    def y_copy(t, index):
        piece = rep if t in SHARED else None
        src = away.at[rows_of(t, piece, 0), :] if t in GU else source(t, 1 - y, piece)
        return remote(src, slot(t, index, piece), y_send.at[t], y_recv.at[t], mate)

    def z_own(t, rr, side):
        index = line(rr, z)
        src = slot(t, index, rep) if rr == 1 or t in GU else source(t, y, rep)
        return remote(
            src, slot(t, index, rep), z_send.at[t], z_recv.at[t, rr, z], along(z + side)
        )

    def z_fwd(t, rr, position, target):
        place = slot(t, line(rr, position), rep)
        return remote(place, place, z_send.at[t], z_recv.at[t, rr, position], along(target))

    def x_copy(t, rr, position, piece, own=False):
        place = slot(t, line(rr, position), piece)
        recv = x_each.at[(OUT, DN).index(t), rr, position] if t in (OUT, DN) else x_recv.at[t]
        return remote(place, place, x_send.at[len(TYPES) if own else t], recv, twin)

    def drain(t, pieces, sem):
        if t in (OUT, DN):
            region = (wo, wd)[t == DN].at[pl.ds(0, pieces // 2)]
        else:
            size = depth // (2 * len(GU) if t in GU else 2)
            region = (wgu if t in GU else (wc, wu, wb)[t]).at[pl.ds(0, pieces * size), :]
        pltpu.make_async_copy(region, region, sem).wait()

    def z_each(t, rr, act):
        for side in (-1, 1):

            @pl.when(jnp.logical_and(z + side >= 0, z + side < n_z))
            def _():
                act(z_own(t, rr, side))

    def start_own(t, rr):
        if rr == 1:
            y_copy(t, line(1, z)).wait_recv()
            if t in SHARED:
                x_copy(t, 1, z, rep, True).start()
        z_each(t, rr, lambda copy: copy.start())

    inner = jnp.minimum(z, n_z - 1 - z) > 0
    outer = jnp.logical_not(inner)

    def relay(t, rr, k):
        position = kth(k)
        onward = z + jnp.where(position < z, 1, -1)
        z_fwd(t, rr, position, z).wait_recv()

        @pl.when(jnp.logical_and(onward >= 0, onward < n_z))
        def _():
            z_fwd(t, rr, position, onward).start()

        x_copy(t, rr, position, rep).start()

    def relay_if(where, t, rr, ks):
        @pl.when(where)
        def _():
            for k in ks:
                relay(t, rr, k)

    beyond = range(3, n_z)

    def x_wait(t, pairs):
        for rr, k in pairs:
            x_copy(t, rr, kth(k), 1 - rep).wait_recv()

    def x_all(t):
        drain(t, 2 * (n_z - 1), x_recv.at[t])


    def half_rows(which, first=0, count=None):
        return pl.ds(pl.multiple_of(which * rows + first, 16), rows if count is None else count)

    def core_copy(src, dst, sems, place, leave=None):
        return remote(src, dst, sems[0].at[place if leave is None else leave], sems[1].at[place], core)

    def mate_copy(src, dst, sems, place, leave=None):
        return remote(src, dst, sems[0].at[place if leave is None else leave], sems[1].at[place], mate)

    one, mix, mid, two = (one_send, one_recv), (mix_send, mix_recv), (mid_send, mid_recv), (two_send, two_recv)
    mine, other = half_rows(tp), half_rows(1 - tp)


    barrier = pltpu.get_barrier_semaphore()
    for device in (core, mate, twin):
        pl.semaphore_signal(barrier, inc=1, device_id=device, device_id_type=MESH)
    neighbours = 3
    for side in (-1, 1):
        inside = jnp.logical_and(z + side >= 0, z + side < n_z)
        neighbours += inside.astype(jnp.int32)

        @pl.when(inside)
        def _(side=side):
            pl.semaphore_signal(barrier, inc=1, device_id=along(z + side), device_id_type=MESH)

    raw = [
        pltpu.make_async_copy(src, dst, load_sem.at[place])
        for src, dst, place in ((tok_hbm, tok, GU[0]), (wg_hbm, raw_gate, GU[1]), (wup_hbm, raw_up, len(TYPES)))
    ]
    raw[0].start()
    pl.semaphore_wait(barrier, neighbours)
    for t in (C, U, B):
        y_copy(t, fs).start()
    for t in (C, U, B):
        start_own(t, 0)
    for copy in raw[1:]:
        copy.start()
    for t in (C, U, B, OUT, DN):
        local(t).start()
    raw[0].wait()

    @pl.loop(0, rows // STRIP)
    def _(i):
        at = pl.ds(pl.multiple_of(i * STRIP, STRIP), STRIP)
        values = f32(tok[at, :])
        factor = lax.rsqrt(jnp.mean(values * values, axis=-1, keepdims=True) + 1e-06)
        normed[0, pl.ds(pl.multiple_of(tp * rows + i * STRIP, STRIP), STRIP), :] = (
            values * factor * gain_one[...]
        ).astype(jnp.bfloat16)

    one_core = core_copy(normed.at[0, mine, :], normed.at[0, mine, :], one, 0)
    one_mate = mate_copy(normed.at[0, mine, :], normed.at[1, mine, :], one, 1)
    one_pass = core_copy(normed.at[1, mine, :], normed.at[1, mine, :], one, 2)
    y_copy(OUT, fs).start()
    one_core.start()
    one_mate.start()

    def relays(types, rr, k):
        for t in types:
            relay(t, rr, k)

    three = (C, U, B)
    relays(three, 0, 1)
    start_own(C, 1)
    for copy in raw[1:]:
        copy.wait()

    @pl.loop(0, depth // STRIP)
    def _(i):
        at = pl.ds(pl.multiple_of(i * STRIP, STRIP), STRIP)
        here = pl.ds(pl.multiple_of(fs * depth + i * STRIP, STRIP), STRIP)
        gate, up = f32(raw_gate[at, :]), f32(raw_up[at, :])
        for half in range(2):
            cut = slice(half * units, (half + 1) * units)
            both = jnp.concatenate([gate[:, cut], up[:, cut]], axis=1).astype(jnp.bfloat16)

            @pl.when(y == half)
            def _(both=both):
                wgu[here, :] = both

            @pl.when(y != half)
            def _(both=both):
                away[at, :] = both

    for t in (*GU, DN):
        y_copy(t, fs).start()


    my_taps = pl.ds(pl.multiple_of((tp * 2 + y) * channels, 128), channels)

    def convolve(seq, half):
        at = pl.ds(half * rows, rows)
        left = normed[seq, at, :]
        mixed = f32(mxu(left, wc[...]).astype(jnp.bfloat16)) * f32(mxu(left, wu[...]).astype(jnp.bfloat16))
        row = lax.broadcasted_iota(jnp.int32, mixed.shape, 0)
        before = [jnp.zeros((1, channels), jnp.float32)] * 2 if half == 0 else [tail[0:1, :], tail[1:2, :]]
        back_one = jnp.where(row == 0, before[1], pltpu.roll(mixed, 1, 0))
        back_two = jnp.where(row == 0, before[0], jnp.where(row == 1, before[1], pltpu.roll(mixed, 2, 0)))
        if half == 0:
            tail[0:2, :] = mixed[rows - 2 : rows, :]
        convolved[seq, at, :] = (
            taps[0:1, my_taps] * back_two + taps[1:2, my_taps] * back_one + taps[2:3, my_taps] * mixed
        )

    def gate_out(seq, half):
        at = pl.ds(half * rows, rows)
        b_proj = f32(mxu(normed[seq, at, :], wb[...]).astype(jnp.bfloat16))
        gated[seq, at, :] = (b_proj * convolved[seq, at, :]).astype(jnp.bfloat16)

    arrivals = sorted((max(k, 2), rr, k) for rr in range(2) for k in range(1, n_z))
    for place, (_, rr, k) in enumerate(arrivals[1:]):
        if place == len(arrivals) - 3:
            start_own(OUT, 0)
        relays(three, rr, k)
        if place == 0:
            start_own(U, 1)
            start_own(B, 1)
    start_own(OUT, 1)
    relay(OUT, 0, 1)
    relay(OUT, 1, 1)
    relay_if(inner, OUT, 0, [2])
    relay_if(inner, OUT, 1, [2])
    one_mate.wait_recv()
    one_pass.start()
    for t in (C, U):
        local(t).wait()
        x_all(t)
    core_copy(normed.at[1, other, :], normed.at[1, other, :], one, 2).wait_recv()

    halves = [pl.ds(i * sub, sub) for i in range(2)]

    def piece(which, i):
        return half_rows(which, i * sub, sub)

    def mix_core(index, i):
        return core_copy(
            part.at[index, 1, piece(1 - tp, i), :], theirs.at[index, 1, halves[i], :], mix, index * 4 + i, 0
        )

    def mix_mate(index, i):
        return mate_copy(outgo.at[index, halves[i], :], income.at[index, halves[i], :], mix, index * 4 + 2 + i, 1)

    def mix_own(index):
        return core_copy(part.at[index, 0, other, :], theirs.at[index, 0], mix, 4 * n_fs, 2)

    def project_out(index, i):
        right = wo[index]
        for which in (1 - tp, tp):
            at = piece(which, i)
            part[index, 1, at, :] = mxu(gated[1, at, :], right).astype(jnp.bfloat16)
            if which is not tp:
                mix_core(index, i).start()

    def project_own(index):
        right = wo[index]
        part[index, 0, other, :] = mxu(gated[0, other, :], right).astype(jnp.bfloat16)
        mix_own(index).start()
        part[index, 0, mine, :] = mxu(gated[0, mine, :], right).astype(jnp.bfloat16)

    def send_sum(index, i):
        mix_core(index, i).wait_recv()
        outgo[index, halves[i], :] = (
            f32(part[index, 1, piece(tp, i), :]) + f32(theirs[index, 1, halves[i], :])
        ).astype(jnp.bfloat16)
        mix_mate(index, i).start()

    order = [line(rr, kth(k)) for k in range(n_z) for rr in range(2)]

    def mix_out(places, i):
        places = list(places)
        for place in places:
            if i == 0 and place > 1:
                x_wait(OUT, [(place % 2, place // 2)])
            project_out(order[place], i)
            if place > places[0]:
                send_sum(order[place - 1], i)
        send_sum(order[places[-1]], i)

    convolve(1, 0)
    relay_if(outer, OUT, 0, [2])
    relay_if(inner, OUT, 0, beyond)
    convolve(1, 1)
    relay_if(outer, OUT, 1, [2])
    relay_if(inner, OUT, 1, beyond)
    for t in GU:
        start_own(t, 0)
    local(B).wait()
    x_all(B)
    gate_out(1, 0)
    gate_out(1, 1)
    local(OUT).wait()
    mix_out(range(2), 0)
    mix_out(range(2, 4), 0)
    for rr in range(2):
        relay_if(outer, OUT, rr, beyond)
    for t in GU:
        start_own(t, 1)
    core_copy(normed.at[0, other, :], normed.at[0, other, :], one, 0).wait_recv()
    todo = [(t, rr, k) for k in range(1, n_z) for rr in range(2) for t in GU]
    todo.reverse()

    def pump(count):
        for _ in range(min(count, len(todo))):
            relay(*todo.pop())

    mix_out(range(4), 1)
    pump(1)
    mix_out(range(4, 6), 0)
    mix_out(range(6, n_fs), 0)
    pump(1)
    mix_out(range(4, n_fs), 1)
    pump(1)
    convolve(0, 0)
    convolve(0, 1)
    pump(1)
    gate_out(0, 0)
    gate_out(0, 1)
    for index in order:
        project_own(index)

    def add_up(index, i):
        mix_mate(index, i).wait_recv()
        at, cols = halves[i], pl.ds(pl.multiple_of(index * width, 128), width)
        res[at, cols] = f32(tok[at, cols]) + (
            (f32(part[index, 0, piece(tp, i), :]) + f32(theirs[index, 0, at, :])) + f32(income[index, at, :])
        )

    strips = sub // STRIP

    def mid_core(which, i):
        return core_copy(normed_two.at[0, piece(which, i), :], normed_two.at[0, piece(which, i), :], mid, i)

    def mid_mate(i):
        return mate_copy(normed_two.at[0, piece(tp, i), :], normed_two.at[1, piece(tp, i), :], mid, 2 + i)

    def mid_pass(which, i):
        return core_copy(normed_two.at[1, piece(which, i), :], normed_two.at[1, piece(which, i), :], mid, 4 + i)

    def norm_two(i):
        if i == 0:
            pltpu.make_async_copy(outgo, outgo, mix_recv.at[4 * n_fs]).wait()
        for index in order:
            add_up(index, i)

        @pl.loop(0, strips)
        def _(j):
            first = i * sub + j * STRIP
            at = pl.ds(pl.multiple_of(first, STRIP), STRIP)
            values = res[at, :]
            factor = lax.rsqrt(jnp.mean(values * values, axis=-1, keepdims=True) + 1e-06)
            normed_two[0, half_rows(tp, first, STRIP), :] = (values * factor * gain_two[...]).astype(jnp.bfloat16)

        mid_mate(i).start()
        mid_core(tp, i).start()

    pump(1)
    norm_two(0)
    pump(2)
    norm_two(1)
    pump(len(todo))
    start_own(DN, 0)
    start_own(DN, 1)


    def feed(seq, at):
        both = mxu(normed_two[seq, at, :], wgu[...])
        gate, up = both[:, :units], both[:, units:]
        hidden[seq, at, :] = (gate / (1.0 + jnp.exp(-gate)) * up).astype(jnp.bfloat16)

    def two_core(index, i):
        return core_copy(
            part_two.at[index, 1, piece(1 - tp, i), :], theirs_two.at[index, 1, halves[i], :], two, index * 4 + i, 0
        )

    def two_mate(index, i):
        return mate_copy(
            outgo_two.at[index, halves[i], :], income_two.at[index, halves[i], :], two, index * 4 + 2 + i, 1
        )

    def two_own(index):
        return core_copy(part_two.at[index, 0, other, :], theirs_two.at[index, 0], two, 4 * n_fs, 2)

    def down(index, i):
        right = wd[index]
        for which in (1 - tp, tp):
            at = piece(which, i)
            part_two[index, 1, at, :] = mxu(hidden[1, at, :], right).astype(jnp.bfloat16)
        two_core(index, i).start()

    def add_cores(index, i):
        two_core(index, i).wait_recv()
        outgo_two[index, halves[i], :] = (
            f32(part_two[index, 1, piece(tp, i), :]) + f32(theirs_two[index, 1, halves[i], :])
        ).astype(jnp.bfloat16)
        two_mate(index, i).start()

    def down_own(index):
        right = wd[index]
        for at in (other, mine):
            part_two[index, 0, at, :] = mxu(hidden[0, at, :], right).astype(jnp.bfloat16)
        two_own(index).start()

    behind = []

    def step(place, i):
        down(order[place], i)
        if behind:
            add_cores(*behind.pop())
        behind.append((order[place], i))

    def flush():
        while behind:
            add_cores(*behind.pop())

    def both_down(place):
        x_wait(DN, [(place % 2, place // 2)])
        step(place, 0)
        step(place, 1)

    mid_mate(0).wait_recv()
    mid_pass(tp, 0).start()
    for t in GU:
        x_all(t)
    relay(DN, 0, 1)
    feed(1, piece(tp, 0))
    relay(DN, 1, 1)
    mid_pass(1 - tp, 0).wait_recv()
    feed(1, piece(1 - tp, 0))
    local(DN).wait()
    if DN in SHARED:
        x_wait(DN, [(1, 0)])
    step(0, 0)
    step(1, 0)
    flush()
    relay(DN, 0, 2)
    mid_mate(1).wait_recv()
    mid_pass(tp, 1).start()
    feed(1, piece(tp, 1))
    mid_pass(1 - tp, 1).wait_recv()
    feed(1, piece(1 - tp, 1))
    step(0, 1)
    step(1, 1)
    flush()
    relay(DN, 1, 2)
    both_down(2)
    both_down(3)
    flush()
    relay_if(inner, DN, 0, beyond)
    feed(0, mine)
    relay_if(inner, DN, 1, beyond)
    both_down(4)
    relay_if(outer, DN, 0, beyond)
    both_down(5)
    flush()
    mid_core(1 - tp, 0).wait_recv()
    mid_core(1 - tp, 1).wait_recv()
    feed(0, other)
    relay_if(outer, DN, 1, beyond)
    for place in range(6, n_fs):
        both_down(place)
        flush()
        down_own(order[place - 6])
    for place in range(n_fs - 6, n_fs):
        down_own(order[place])
    pltpu.make_async_copy(outgo_two, outgo_two, two_recv.at[4 * n_fs]).wait()
    for index in order:
        for i in range(2):
            two_mate(index, i).wait_recv()
        cols = pl.ds(pl.multiple_of(index * width, 128), width)
        total = (f32(part_two[index, 0, mine, :]) + f32(theirs_two[index, 0])) + f32(income_two[index])
        final[:, cols] = (res[:, cols] + 0.5 * total).astype(jnp.bfloat16)


    for t in TYPES:
        y_copy(t, fs).wait_send()
        drain(t, 2 * (n_z - 1), x_send.at[t])

        @pl.when(inner)
        def _(t=t):
            drain(t, 4 + 2 * (n_z - 1), z_send.at[t])

        @pl.when(outer)
        def _(t=t):
            drain(t, 2, z_send.at[t])

        if t in SHARED:
            x_copy(t, 1, z, rep, True).wait_send()
    for send, whole in ((mix_send, outgo), (two_send, outgo_two)):
        for place in range(3):
            pltpu.make_async_copy(whole, whole, send.at[place]).wait()
    sent = [one_core, one_mate, one_pass]
    sent += [make for i in range(2) for make in (mid_core(tp, i), mid_mate(i), mid_pass(tp, i))]
    for copy in sent:
        copy.wait_send()


def block(
    n_fs, tokens, mix_gain, w_bgate, w_cgate, w_value, conv_taps, w_mixout, mlp_gain, w_gate, w_up, w_down
):
    rows, dim = tokens.shape
    depth, channels = w_bgate.shape[0], w_bgate.shape[1] // 2
    units = w_gate.shape[1] // 2
    width = w_mixout.shape[1]
    n_z = n_fs // 2
    bf16 = jnp.bfloat16
    hbm = pl.BlockSpec(memory_space=pl.ANY)
    vmem = pl.BlockSpec(memory_space=pltpu.VMEM)
    dma = pltpu.SemaphoreType.DMA
    return pl.pallas_call(
        functools.partial(kernel, n_z),
        out_shape=pltpu.VMEM(tokens.shape, tokens.dtype),
        in_specs=[hbm, vmem, hbm, hbm, hbm, vmem, hbm, vmem, hbm, hbm, hbm],
        out_specs=vmem,
        scratch_shapes=[
            *[pltpu.VMEM((n_fs * depth, channels), bf16)] * 3,
            pltpu.VMEM((n_fs, w_mixout.shape[0] // 2, width), bf16),
            pltpu.VMEM((n_fs * depth, 2 * units), bf16),
            pltpu.VMEM((n_fs, w_down.shape[0] // 2, width), bf16),
            *[pltpu.VMEM((depth, 2 * units), bf16)] * 3,
            pltpu.VMEM((rows, dim), bf16),
            pltpu.VMEM((2, 2 * rows, dim), bf16),
            pltpu.VMEM((2, 2 * rows, channels), jnp.float32),
            pltpu.VMEM((2, 2 * rows, channels), bf16),
            pltpu.VMEM((n_fs, 2, 2 * rows, width), bf16),
            pltpu.VMEM((n_fs, 2, rows, width), bf16),
            pltpu.VMEM((n_fs, rows, width), bf16),
            pltpu.VMEM((n_fs, rows, width), bf16),
            pltpu.VMEM((rows, dim), jnp.float32),
            pltpu.VMEM((2, 2 * rows, dim), bf16),
            pltpu.VMEM((2, 2 * rows, units), bf16),
            pltpu.VMEM((n_fs, 2, 2 * rows, width), bf16),
            pltpu.VMEM((n_fs, 2, rows, width), bf16),
            pltpu.VMEM((n_fs, rows, width), bf16),
            pltpu.VMEM((n_fs, rows, width), bf16),
            pltpu.VMEM((8, channels), jnp.float32),
            dma((len(TYPES) + 1,)),
            *[dma((len(TYPES),))] * 3,
            dma((len(TYPES), 2, n_z)),
            dma((len(TYPES) + 1,)),
            dma((len(TYPES),)),
            dma((2, 2, n_z)),
            *[dma((3,))] * 2,
            *[dma((3,)), dma((4 * n_fs + 1,))],
            *[dma((6,))] * 2,
            *[dma((3,)), dma((4 * n_fs + 1,))],
        ],
        compiler_params=pltpu.CompilerParams(
            collective_id=0, has_side_effects=True, vmem_limit_bytes=64_500_000
        ),
    )(
        tokens, mix_gain[None], w_bgate, w_cgate, w_value, conv_taps, w_mixout, mlp_gain[None], w_gate, w_up, w_down
    )


SPECS = (
    P(("rep", "fs", "tp"), None),
    P(),
    P("fs", "tp"),
    P("fs", "tp"),
    P("fs", "tp"),
    P(),
    P("tp", "fs"),
    P(),
    P("fs", "tp"),
    P("fs", "tp"),
    P("tp", "fs"),
)


def permuted(mesh):
    return jax.shard_map(
        build(mesh.shape["fs"]),
        mesh=mesh,
        in_specs=SPECS,
        out_specs=P(("rep", "fs", "tp"), None),
        check_vma=False,
    )


def fused(mesh):
    return jax.shard_map(
        functools.partial(block, mesh.shape["fs"]),
        mesh=mesh,
        in_specs=SPECS,
        out_specs=P(("rep", "fs", "tp"), None),
        check_vma=False,
    )


def solution(mesh):
    n_fs, n_rep, n_tp = (mesh.shape[name] for name in ("fs", "rep", "tp"))

    def step(*operands):
        tokens, w_down = operands[0], operands[-1]
        rows = tokens.shape[0] // (n_rep * n_fs * n_tp)
        width = tokens.shape[1] // n_fs
        units = w_down.shape[0] // n_tp
        aligned = (
            (n_rep, n_tp, n_fs % 2) == (2, 2, 0)
            and (rows % (2 * STRIP), width % LANES, units % (4 * STRIP), units % LANES) == (0, 0, 0, 0)
            and tokens.shape[1] % (4 * LANES) == 0
        )
        return (fused if aligned else permuted)(mesh)(*operands)

    return step
```

```python
import functools

import jax
import jax.numpy as jnp
from jax import lax
from jax.experimental import pallas as pl
from jax.experimental.pallas import tpu as pltpu
from jax.sharding import PartitionSpec as P


def rms_scale(matrix, gain):
    values = matrix.astype(jnp.float32)
    factor = lax.rsqrt(jnp.mean(values * values, axis=-1, keepdims=True) + 1e-06)
    return values * factor * gain


def causal_taps(mixed, filters):
    length = mixed.shape[-2]
    padded = jnp.pad(mixed, [(2, 0), (0, 0)])
    return (
        filters[0] * padded[0:length]
        + filters[1] * padded[1 : length + 1]
        + filters[2] * padded[2 : length + 2]
    )


def swap(array, axis):
    return lax.ppermute(array, axis, [(0, 1), (1, 0)])


def half(array, axis, part):
    size = array.shape[axis] // 2
    return lax.dynamic_slice_in_dim(array, part * size, size, axis)


def build(n_fs):
    ring = [(i, (i + 2) % n_fs) for i in range(n_fs)]
    pair = [(i, i ^ 1) for i in range(n_fs)]
    steps = n_fs // 2

    def ring_first(block):
        blocks = []
        for step in range(steps):
            blocks += [block, lax.ppermute(block, "fs", pair)]
            if step < steps - 1:
                block = lax.ppermute(block, "fs", ring)
        return blocks

    def pair_first(block):
        mate = lax.ppermute(block, "fs", pair)
        blocks = []
        for step in range(steps):
            blocks += [block, mate]
            if step < steps - 1:
                block = lax.ppermute(block, "fs", ring)
                mate = lax.ppermute(mate, "fs", ring)
        return blocks

    def on_device(
        tokens, mix_gain, w_bgate, w_cgate, w_value, conv_taps, w_mixout, mlp_gain, w_gate, w_up, w_down
    ):
        rep, fs, tp = (lax.axis_index(name) for name in ("rep", "fs", "tp"))
        width = tokens.shape[1] // n_fs

        def arrival_order(array):
            order = [((fs ^ j) - 2 * s + n_fs) % n_fs for s in range(steps) for j in range(2)]
            return jnp.concatenate(
                [lax.dynamic_slice_in_dim(array, k * width, width, array.ndim - 1) for k in order],
                axis=-1,
            )

        def global_order(array):
            places = []
            for k in range(n_fs):
                j = (fs ^ k) & 1
                places.append((((fs ^ j) - k + n_fs) % n_fs) + j)
            return jnp.concatenate(
                [lax.dynamic_slice_in_dim(array, k * width, width, array.ndim - 1) for k in places],
                axis=-1,
            )

        def sequence(rows):
            other = swap(rows, "tp")
            return jnp.concatenate(
                [jnp.where(tp == 0, rows, other), jnp.where(tp == 0, other, rows)], axis=0
            )

        def both_sequences(rows):
            away = swap(rows, "rep")
            return sequence(rows), sequence(away)

        def chip_sum(partial):
            other = swap(half(partial, 0, 1 - tp), "tp")
            return half(partial, 0, tp).astype(jnp.float32) + other.astype(jnp.float32)

        def project_out(mine, theirs, blocks, group):
            sums = []
            for start in range(0, len(blocks), group):
                weight = jnp.concatenate(blocks[start : start + group], axis=1)
                outs = []
                for rows in (theirs, mine):
                    outs.append(
                        jnp.dot(rows, weight, preferred_element_type=jnp.float32).astype(
                            jnp.bfloat16
                        )
                    )
                away = swap(chip_sum(outs[0]).astype(jnp.bfloat16), "rep")
                sums.append(chip_sum(outs[1]) + away.astype(jnp.float32))
            return jnp.concatenate(sums, axis=1)

        w_in = jnp.concatenate([half(w, 1, rep) for w in (w_bgate, w_cgate, w_value)], axis=1)
        w_gu = jnp.concatenate([half(w, 1, rep) for w in (w_gate, w_up)], axis=1)
        in_blocks = ring_first(w_in)
        out_blocks = ring_first(half(w_mixout, 0, rep))
        upper, lower = jnp.split(w_gu, 2, axis=0)
        gu_blocks = [part for both in zip(pair_first(upper), ring_first(lower)) for part in both]
        down_blocks = ring_first(half(w_down, 0, rep))

        channels = w_in.shape[1] // 3
        taps = lax.dynamic_slice_in_dim(conv_taps, (tp * 2 + rep) * channels, channels, 1)
        local = arrival_order(tokens)

        def mix(normed, weight):
            projected = jnp.dot(normed, weight, preferred_element_type=jnp.float32).astype(
                jnp.bfloat16
            )
            b_proj, c_proj, u_proj = (
                projected[:, k * channels : (k + 1) * channels].astype(jnp.float32)
                for k in range(3)
            )
            return (b_proj * causal_taps(c_proj * u_proj, taps)).astype(jnp.bfloat16)

        mine, theirs = both_sequences(rms_scale(local, arrival_order(mix_gain)).astype(jnp.bfloat16))
        weight = jnp.concatenate(in_blocks, axis=0)
        theirs, mine = mix(theirs, weight), mix(mine, weight)
        mixed = project_out(mine, theirs, out_blocks, 2)
        residual = local.astype(jnp.float32) + mixed

        units = w_gu.shape[1] // 2

        def feed(normed, weight):
            both = jnp.dot(normed, weight, preferred_element_type=jnp.float32)
            return (jax.nn.silu(both[:, :units]) * both[:, units:]).astype(jnp.bfloat16)

        mine, theirs = both_sequences(rms_scale(residual, arrival_order(mlp_gain)).astype(jnp.bfloat16))
        weight = jnp.concatenate(gu_blocks, axis=0)
        theirs, mine = feed(theirs, weight), feed(mine, weight)
        down = project_out(mine, theirs, down_blocks, 2)
        return global_order((residual + 0.5 * down).astype(jnp.bfloat16))

    return on_device


MESH = pl.DeviceIdType.MESH
STRIP = 16
LANES = 128
C, U, B, OUT, *GU, DN = TYPES = range(9)
SHARED = (DN,)


def f32(value):
    return value.astype(jnp.float32)


def mxu(left, right):
    return jnp.dot(left, right, preferred_element_type=jnp.float32)


def kernel(
    n_z,
    tok_hbm, gain_one, wb_hbm, wc_hbm, wu_hbm, taps, wo_hbm, gain_two, wg_hbm, wup_hbm, wd_hbm,
    final,
    wb, wc, wu, wo, wgu, wd,
    raw_gate, raw_up, away,
    tok, normed, convolved, gated, part, theirs, outgo, income, res, normed_two, hidden,
    part_two, theirs_two, outgo_two, income_two,
    tail,
    load_sem, y_send, y_recv, z_send, z_recv, x_send, x_recv, x_each,
    one_send, one_recv, mix_send, mix_recv, mid_send, mid_recv, two_send, two_recv,
):
    rep, fs, tp = (lax.axis_index(name) for name in ("rep", "fs", "tp"))
    z, y = lax.div(fs, 2), lax.rem(fs, 2)
    rows, _ = tok.shape
    sub = rows // 2
    depth = wb_hbm.shape[0]
    channels = wb.shape[1]
    pair_units = wgu.shape[1]
    units = pair_units // 2
    width = wo.shape[2]
    n_fs = 2 * n_z
    core = (rep, fs, 1 - tp)
    mate = (rep, z * 2 + 1 - y, tp)
    twin = (1 - rep, fs, tp)

    def along(position):
        return (rep, position * 2 + y, tp)

    def kth(k):
        near = jnp.minimum(z, n_z - 1 - z)
        longer = jnp.where(z < n_z - 1 - z, 1, -1)
        both = z + longer * (((k + 1) // 2) * (1 if k % 2 == 1 else -1))
        return jnp.where(k <= 2 * near, both, z + longer * (k - near))

    def line(rr, position):
        return position * 2 + (y if rr == 0 else 1 - y)

    def rows_of(t, piece, base):
        if t in (OUT, DN):
            size = (wo, wd)[t == DN].shape[1] // 2
        else:
            size = depth // (2 * len(GU) if t in GU else 2)
        first = base + (2 * size * GU.index(t) if t in GU else 0)
        if piece is None:
            return pl.ds(pl.multiple_of(first, 16), 2 * size)
        return pl.ds(pl.multiple_of(first + piece * size, 16), size)

    def source(t, half, piece=None):
        if t in (OUT, DN):
            ref = (wo_hbm, wd_hbm)[t == DN]
            return ref.at[rows_of(t, piece, half * (ref.shape[0] // 2)), :]
        ref = (wc_hbm, wu_hbm, wb_hbm)[t]
        return ref.at[rows_of(t, piece, 0), pl.ds(pl.multiple_of(half * channels, 128), channels)]

    def slot(t, index, piece=None):
        if t in (OUT, DN):
            return (wo, wd)[t == DN].at[index, rows_of(t, piece, 0), :]
        return (wgu if t in GU else (wc, wu, wb)[t]).at[rows_of(t, piece, index * depth), :]

    def remote(src, dst, send, recv, device):
        return pltpu.make_async_remote_copy(
            src_ref=src, dst_ref=dst, send_sem=send, recv_sem=recv, device_id=device, device_id_type=MESH
        )


    def local(t):
        return pltpu.make_async_copy(source(t, y), slot(t, fs), load_sem.at[t])

    def y_copy(t, index):
        piece = rep if t in SHARED else None
        src = away.at[rows_of(t, piece, 0), :] if t in GU else source(t, 1 - y, piece)
        return remote(src, slot(t, index, piece), y_send.at[t], y_recv.at[t], mate)

    def z_own(t, rr, side):
        index = line(rr, z)
        src = slot(t, index, rep) if rr == 1 or t in GU else source(t, y, rep)
        return remote(
            src, slot(t, index, rep), z_send.at[t], z_recv.at[t, rr, z - (side < 0)], along(z + side)
        )

    def z_fwd(t, rr, position, target):
        place = slot(t, line(rr, position), rep)
        return remote(place, place, z_send.at[t], z_recv.at[t, rr, position - (position > target).astype(jnp.int32)], along(target))

    def x_copy(t, rr, position, piece, own=False):
        place = slot(t, line(rr, position), piece)
        recv = x_each.at[(OUT, DN).index(t), rr, position] if t in (OUT, DN) else x_recv.at[t]
        return remote(place, place, x_send.at[len(TYPES) if own else t], recv, twin)

    def drain(t, pieces, sem):
        if t in (OUT, DN):
            region = (wo, wd)[t == DN].at[pl.ds(0, pieces // 2)]
        else:
            size = depth // (2 * len(GU) if t in GU else 2)
            region = (wgu if t in GU else (wc, wu, wb)[t]).at[pl.ds(0, pieces * size), :]
        pltpu.make_async_copy(region, region, sem).wait()

    def z_each(t, rr, act):
        for side in (-1, 1):

            @pl.when(jnp.logical_and(z + side >= 0, z + side < n_z))
            def _():
                act(z_own(t, rr, side))

    def start_own(t, rr):
        if rr == 1:
            y_copy(t, line(1, z)).wait_recv()
            if t in SHARED:
                x_copy(t, 1, z, rep, True).start()
        z_each(t, rr, lambda copy: copy.start())

    inner = jnp.minimum(z, n_z - 1 - z) > 0
    outer = jnp.logical_not(inner)

    def relay(t, rr, k):
        position = kth(k)
        onward = z + jnp.where(position < z, 1, -1)
        z_fwd(t, rr, position, z).wait_recv()

        @pl.when(jnp.logical_and(onward >= 0, onward < n_z))
        def _():
            z_fwd(t, rr, position, onward).start()

        x_copy(t, rr, position, rep).start()

    def relay_if(where, t, rr, ks):
        @pl.when(where)
        def _():
            for k in ks:
                relay(t, rr, k)

    beyond = range(3, n_z)

    def x_wait(t, pairs):
        for rr, k in pairs:
            x_copy(t, rr, kth(k), 1 - rep).wait_recv()

    def x_all(t):
        drain(t, 2 * (n_z - 1), x_recv.at[t])


    def half_rows(which, first=0, count=None):
        return pl.ds(pl.multiple_of(which * rows + first, 16), rows if count is None else count)

    def core_copy(src, dst, sems, place, leave=None):
        return remote(src, dst, sems[0].at[place if leave is None else leave], sems[1].at[place], core)

    def mate_copy(src, dst, sems, place, leave=None):
        return remote(src, dst, sems[0].at[place if leave is None else leave], sems[1].at[place], mate)

    one, mix, mid, two = (one_send, one_recv), (mix_send, mix_recv), (mid_send, mid_recv), (two_send, two_recv)
    mine, other = half_rows(tp), half_rows(1 - tp)


    barrier = pltpu.get_barrier_semaphore()
    for device in (core, mate, twin):
        pl.semaphore_signal(barrier, inc=1, device_id=device, device_id_type=MESH)
    neighbours = 3
    for side in (-1, 1):
        inside = jnp.logical_and(z + side >= 0, z + side < n_z)
        neighbours += inside.astype(jnp.int32)

        @pl.when(inside)
        def _(side=side):
            pl.semaphore_signal(barrier, inc=1, device_id=along(z + side), device_id_type=MESH)

    raw = [
        pltpu.make_async_copy(src, dst, load_sem.at[place])
        for src, dst, place in ((tok_hbm, tok, GU[0]), (wg_hbm, raw_gate, GU[1]), (wup_hbm, raw_up, len(TYPES)))
    ]
    raw[0].start()
    pl.semaphore_wait(barrier, neighbours)
    for t in (C, U, B):
        y_copy(t, fs).start()
    for t in (C, U, B):
        start_own(t, 0)
    for copy in raw[1:]:
        copy.start()
    for t in (C, U, B, OUT, DN):
        local(t).start()
    raw[0].wait()

    @pl.loop(0, rows // STRIP)
    def _(i):
        at = pl.ds(pl.multiple_of(i * STRIP, STRIP), STRIP)
        values = f32(tok[at, :])
        factor = lax.rsqrt(jnp.mean(values * values, axis=-1, keepdims=True) + 1e-06)
        normed[0, pl.ds(pl.multiple_of(tp * rows + i * STRIP, STRIP), STRIP), :] = (
            values * factor * gain_one[...]
        ).astype(jnp.bfloat16)

    one_core = core_copy(normed.at[0, mine, :], normed.at[0, mine, :], one, 0)
    one_mate = mate_copy(normed.at[0, mine, :], normed.at[1, mine, :], one, 1)
    one_pass = core_copy(normed.at[1, mine, :], normed.at[1, mine, :], one, 2)
    y_copy(OUT, fs).start()
    one_core.start()
    one_mate.start()

    def relays(types, rr, k):
        for t in types:
            relay(t, rr, k)

    three = (C, U, B)
    relays(three, 0, 1)
    start_own(C, 1)
    for copy in raw[1:]:
        copy.wait()

    @pl.loop(0, depth // STRIP)
    def _(i):
        at = pl.ds(pl.multiple_of(i * STRIP, STRIP), STRIP)
        here = pl.ds(pl.multiple_of(fs * depth + i * STRIP, STRIP), STRIP)
        gate, up = f32(raw_gate[at, :]), f32(raw_up[at, :])
        for half in range(2):
            cut = slice(half * units, (half + 1) * units)
            both = jnp.concatenate([gate[:, cut], up[:, cut]], axis=1).astype(jnp.bfloat16)

            @pl.when(y == half)
            def _(both=both):
                wgu[here, :] = both

            @pl.when(y != half)
            def _(both=both):
                away[at, :] = both

    for t in (*GU, DN):
        y_copy(t, fs).start()


    my_taps = pl.ds(pl.multiple_of((tp * 2 + y) * channels, 128), channels)

    def convolve(seq, half):
        at = pl.ds(half * rows, rows)
        left = normed[seq, at, :]
        mixed = f32(mxu(left, wc[...]).astype(jnp.bfloat16)) * f32(mxu(left, wu[...]).astype(jnp.bfloat16))
        row = lax.broadcasted_iota(jnp.int32, mixed.shape, 0)
        before = [jnp.zeros((1, channels), jnp.float32)] * 2 if half == 0 else [tail[0:1, :], tail[1:2, :]]
        back_one = jnp.where(row == 0, before[1], pltpu.roll(mixed, 1, 0))
        back_two = jnp.where(row == 0, before[0], jnp.where(row == 1, before[1], pltpu.roll(mixed, 2, 0)))
        if half == 0:
            tail[0:2, :] = mixed[rows - 2 : rows, :]
        convolved[seq, at, :] = (
            taps[0:1, my_taps] * back_two + taps[1:2, my_taps] * back_one + taps[2:3, my_taps] * mixed
        )

    def gate_out(seq, half):
        at = pl.ds(half * rows, rows)
        b_proj = f32(mxu(normed[seq, at, :], wb[...]).astype(jnp.bfloat16))
        gated[seq, at, :] = (b_proj * convolved[seq, at, :]).astype(jnp.bfloat16)

    arrivals = sorted((max(k, 2), rr, k) for rr in range(2) for k in range(1, n_z))
    for place, (_, rr, k) in enumerate(arrivals[1:]):
        if place == len(arrivals) - 3:
            start_own(OUT, 0)
        relays(three, rr, k)
        if place == 0:
            start_own(U, 1)
            start_own(B, 1)
    start_own(OUT, 1)
    relay(OUT, 0, 1)
    relay(OUT, 1, 1)
    relay_if(inner, OUT, 0, [2])
    relay_if(inner, OUT, 1, [2])
    one_mate.wait_recv()
    one_pass.start()
    for t in (C, U):
        local(t).wait()
        x_all(t)
    core_copy(normed.at[1, other, :], normed.at[1, other, :], one, 2).wait_recv()

    halves = [pl.ds(i * sub, sub) for i in range(2)]

    def piece(which, i):
        return half_rows(which, i * sub, sub)

    def mix_core(index, i):
        return core_copy(
            part.at[index, 1, piece(1 - tp, i), :], theirs.at[index, 1, halves[i], :], mix, index * 4 + i, 0
        )

    def mix_mate(index, i):
        return mate_copy(outgo.at[index, halves[i], :], income.at[index, halves[i], :], mix, index * 4 + 2 + i, 1)

    def mix_own(index):
        return core_copy(part.at[index, 0, other, :], theirs.at[index, 0], mix, 4 * n_fs, 2)

    def project_out(index, i):
        right = wo[index]
        for which in (1 - tp, tp):
            at = piece(which, i)
            part[index, 1, at, :] = mxu(gated[1, at, :], right).astype(jnp.bfloat16)
            if which is not tp:
                mix_core(index, i).start()

    def project_own(index):
        right = wo[index]
        part[index, 0, other, :] = mxu(gated[0, other, :], right).astype(jnp.bfloat16)
        mix_own(index).start()
        part[index, 0, mine, :] = mxu(gated[0, mine, :], right).astype(jnp.bfloat16)

    def send_sum(index, i):
        mix_core(index, i).wait_recv()
        outgo[index, halves[i], :] = (
            f32(part[index, 1, piece(tp, i), :]) + f32(theirs[index, 1, halves[i], :])
        ).astype(jnp.bfloat16)
        mix_mate(index, i).start()

    order = [line(rr, kth(k)) for k in range(n_z) for rr in range(2)]

    def mix_out(places, i):
        places = list(places)
        for place in places:
            if i == 0 and place > 1:
                x_wait(OUT, [(place % 2, place // 2)])
            project_out(order[place], i)
            if place > places[0]:
                send_sum(order[place - 1], i)
        send_sum(order[places[-1]], i)

    convolve(1, 0)
    relay_if(outer, OUT, 0, [2])
    relay_if(inner, OUT, 0, beyond)
    convolve(1, 1)
    relay_if(outer, OUT, 1, [2])
    relay_if(inner, OUT, 1, beyond)
    for t in GU:
        start_own(t, 0)
    local(B).wait()
    x_all(B)
    gate_out(1, 0)
    gate_out(1, 1)
    local(OUT).wait()
    mix_out(range(2), 0)
    relay_if(outer, OUT, 0, beyond)
    mix_out(range(2, 4), 0)
    relay_if(outer, OUT, 1, beyond)
    for t in GU:
        start_own(t, 1)
    core_copy(normed.at[0, other, :], normed.at[0, other, :], one, 0).wait_recv()
    todo = [(t, rr, k) for k in range(1, n_z) for rr in range(2) for t in GU]
    todo = [(inner, todo[::-1]), (outer, todo[::-1])]

    def pump(*counts):
        for (where, left), count in zip(todo, counts):
            items = [left.pop() for _ in range(min(count, len(left)))]

            @pl.when(where)
            def _(items=items):
                for item in items:
                    relay(*item)

    mix_out(range(4), 1)
    pump(1, 1)
    mix_out(range(4, 6), 0)
    pump(1, 1)
    mix_out(range(6, n_fs), 0)
    pump(1, 1)
    mix_out(range(4, n_fs), 1)
    pump(2, 2)
    convolve(0, 0)
    pump(1, 1)
    convolve(0, 1)
    pump(2, 1)
    gate_out(0, 0)
    gate_out(0, 1)
    pump(3, 1)
    for index in order:
        project_own(index)

    def add_up(index, i):
        mix_mate(index, i).wait_recv()
        at, cols = halves[i], pl.ds(pl.multiple_of(index * width, 128), width)
        res[at, cols] = f32(tok[at, cols]) + (
            (f32(part[index, 0, piece(tp, i), :]) + f32(theirs[index, 0, at, :])) + f32(income[index, at, :])
        )

    strips = sub // STRIP

    def mid_core(which, i):
        return core_copy(normed_two.at[0, piece(which, i), :], normed_two.at[0, piece(which, i), :], mid, i)

    def mid_mate(i):
        return mate_copy(normed_two.at[0, piece(tp, i), :], normed_two.at[1, piece(tp, i), :], mid, 2 + i)

    def mid_pass(which, i):
        return core_copy(normed_two.at[1, piece(which, i), :], normed_two.at[1, piece(which, i), :], mid, 4 + i)

    def norm_two(i, relays_after):
        if i == 0:
            pltpu.make_async_copy(outgo, outgo, mix_recv.at[4 * n_fs]).wait()
        for place, index in enumerate(order):
            add_up(index, i)
            if place in relays_after:
                pump(1, 1)

        @pl.loop(0, strips)
        def _(j):
            first = i * sub + j * STRIP
            at = pl.ds(pl.multiple_of(first, STRIP), STRIP)
            values = res[at, :]
            factor = lax.rsqrt(jnp.mean(values * values, axis=-1, keepdims=True) + 1e-06)
            normed_two[0, half_rows(tp, first, STRIP), :] = (values * factor * gain_two[...]).astype(jnp.bfloat16)

        mid_mate(i).start()
        mid_core(tp, i).start()

    pump(5, 1)
    norm_two(0, [4])
    pump(1, 1)
    norm_two(1, range(n_fs - 1))
    rest = len(GU) * 2 * (n_z - 1)
    pump(rest, rest)
    start_own(DN, 0)
    start_own(DN, 1)


    def feed(seq, at):
        both = mxu(normed_two[seq, at, :], wgu[...])
        gate, up = both[:, :units], both[:, units:]
        hidden[seq, at, :] = (gate / (1.0 + jnp.exp(-gate)) * up).astype(jnp.bfloat16)

    def two_core(index, i):
        return core_copy(
            part_two.at[index, 1, piece(1 - tp, i), :], theirs_two.at[index, 1, halves[i], :], two, index * 4 + i, 0
        )

    def two_mate(index, i):
        return mate_copy(
            outgo_two.at[index, halves[i], :], income_two.at[index, halves[i], :], two, index * 4 + 2 + i, 1
        )

    def two_own(index):
        return core_copy(part_two.at[index, 0, other, :], theirs_two.at[index, 0], two, 4 * n_fs, 2)

    def down(index, i):
        right = wd[index]
        for which in (1 - tp, tp):
            at = piece(which, i)
            part_two[index, 1, at, :] = mxu(hidden[1, at, :], right).astype(jnp.bfloat16)
        two_core(index, i).start()

    def add_cores(index, i):
        two_core(index, i).wait_recv()
        outgo_two[index, halves[i], :] = (
            f32(part_two[index, 1, piece(tp, i), :]) + f32(theirs_two[index, 1, halves[i], :])
        ).astype(jnp.bfloat16)
        two_mate(index, i).start()

    def down_own(index):
        right = wd[index]
        for at in (other, mine):
            part_two[index, 0, at, :] = mxu(hidden[0, at, :], right).astype(jnp.bfloat16)
        two_own(index).start()

    behind = []

    def step(place, i):
        down(order[place], i)
        if behind:
            add_cores(*behind.pop())
        behind.append((order[place], i))

    def flush():
        while behind:
            add_cores(*behind.pop())

    def both_down(place):
        x_wait(DN, [(place % 2, place // 2)])
        step(place, 0)
        step(place, 1)

    mid_mate(0).wait_recv()
    mid_pass(tp, 0).start()
    for t in GU:
        x_all(t)
    relay(DN, 0, 1)
    feed(1, piece(tp, 0))
    relay(DN, 1, 1)
    mid_pass(1 - tp, 0).wait_recv()
    feed(1, piece(1 - tp, 0))
    local(DN).wait()
    if DN in SHARED:
        x_wait(DN, [(1, 0)])
    step(0, 0)
    step(1, 0)
    flush()
    relay(DN, 0, 2)
    mid_mate(1).wait_recv()
    mid_pass(tp, 1).start()
    feed(1, piece(tp, 1))
    mid_pass(1 - tp, 1).wait_recv()
    feed(1, piece(1 - tp, 1))
    step(0, 1)
    step(1, 1)
    flush()
    relay(DN, 1, 2)
    both_down(2)
    both_down(3)
    flush()
    relay_if(inner, DN, 0, beyond)
    feed(0, mine)
    relay_if(inner, DN, 1, beyond)
    both_down(4)
    relay_if(outer, DN, 0, beyond)
    both_down(5)
    flush()
    mid_core(1 - tp, 0).wait_recv()
    mid_core(1 - tp, 1).wait_recv()
    feed(0, other)
    relay_if(outer, DN, 1, beyond)
    for place in range(6, n_fs):
        both_down(place)
        flush()
        down_own(order[place - 6])
    for place in range(n_fs - 6, n_fs):
        down_own(order[place])
    pltpu.make_async_copy(outgo_two, outgo_two, two_recv.at[4 * n_fs]).wait()
    for index in order:
        for i in range(2):
            two_mate(index, i).wait_recv()
        cols = pl.ds(pl.multiple_of(index * width, 128), width)
        total = (f32(part_two[index, 0, mine, :]) + f32(theirs_two[index, 0])) + f32(income_two[index])
        final[:, cols] = (res[:, cols] + 0.5 * total).astype(jnp.bfloat16)


    for t in TYPES:
        y_copy(t, fs).wait_send()
        drain(t, 2 * (n_z - 1), x_send.at[t])

        @pl.when(inner)
        def _(t=t):
            drain(t, 4 + 2 * (n_z - 1), z_send.at[t])

        @pl.when(outer)
        def _(t=t):
            drain(t, 2, z_send.at[t])

        if t in SHARED:
            x_copy(t, 1, z, rep, True).wait_send()
    for send, whole in ((mix_send, outgo), (two_send, outgo_two)):
        for place in range(3):
            pltpu.make_async_copy(whole, whole, send.at[place]).wait()
    sent = [one_core, one_mate, one_pass]
    sent += [make for i in range(2) for make in (mid_core(tp, i), mid_mate(i), mid_pass(tp, i))]
    for copy in sent:
        copy.wait_send()


def block(
    n_fs, tokens, mix_gain, w_bgate, w_cgate, w_value, conv_taps, w_mixout, mlp_gain, w_gate, w_up, w_down
):
    rows, dim = tokens.shape
    depth, channels = w_bgate.shape[0], w_bgate.shape[1] // 2
    units = w_gate.shape[1] // 2
    width = w_mixout.shape[1]
    n_z = n_fs // 2
    bf16 = jnp.bfloat16
    hbm = pl.BlockSpec(memory_space=pl.ANY)
    vmem = pl.BlockSpec(memory_space=pltpu.VMEM)
    dma = pltpu.SemaphoreType.DMA
    return pl.pallas_call(
        functools.partial(kernel, n_z),
        out_shape=pltpu.VMEM(tokens.shape, tokens.dtype),
        in_specs=[hbm, vmem, hbm, hbm, hbm, vmem, hbm, vmem, hbm, hbm, hbm],
        out_specs=vmem,
        scratch_shapes=[
            *[pltpu.VMEM((n_fs * depth, channels), bf16)] * 3,
            pltpu.VMEM((n_fs, w_mixout.shape[0] // 2, width), bf16),
            pltpu.VMEM((n_fs * depth, 2 * units), bf16),
            pltpu.VMEM((n_fs, w_down.shape[0] // 2, width), bf16),
            *[pltpu.VMEM((depth, 2 * units), bf16)] * 3,
            pltpu.VMEM((rows, dim), bf16),
            pltpu.VMEM((2, 2 * rows, dim), bf16),
            pltpu.VMEM((2, 2 * rows, channels), jnp.float32),
            pltpu.VMEM((2, 2 * rows, channels), bf16),
            pltpu.VMEM((n_fs, 2, 2 * rows, width), bf16),
            pltpu.VMEM((n_fs, 2, rows, width), bf16),
            pltpu.VMEM((n_fs, rows, width), bf16),
            pltpu.VMEM((n_fs, rows, width), bf16),
            pltpu.VMEM((rows, dim), jnp.float32),
            pltpu.VMEM((2, 2 * rows, dim), bf16),
            pltpu.VMEM((2, 2 * rows, units), bf16),
            pltpu.VMEM((n_fs, 2, 2 * rows, width), bf16),
            pltpu.VMEM((n_fs, 2, rows, width), bf16),
            pltpu.VMEM((n_fs, rows, width), bf16),
            pltpu.VMEM((n_fs, rows, width), bf16),
            pltpu.VMEM((8, channels), jnp.float32),
            dma((len(TYPES) + 1,)),
            *[dma((len(TYPES),))] * 3,
            dma((len(TYPES), 2, n_z - 1)),
            dma((len(TYPES) + 1,)),
            dma((len(TYPES),)),
            dma((2, 2, n_z)),
            *[dma((3,))] * 2,
            *[dma((3,)), dma((4 * n_fs + 1,))],
            *[dma((6,))] * 2,
            *[dma((3,)), dma((4 * n_fs + 1,))],
        ],
        compiler_params=pltpu.CompilerParams(
            collective_id=0, has_side_effects=True, vmem_limit_bytes=64_500_000
        ),
    )(
        tokens, mix_gain[None], w_bgate, w_cgate, w_value, conv_taps, w_mixout, mlp_gain[None], w_gate, w_up, w_down
    )


SPECS = (
    P(("rep", "fs", "tp"), None),
    P(),
    P("fs", "tp"),
    P("fs", "tp"),
    P("fs", "tp"),
    P(),
    P("tp", "fs"),
    P(),
    P("fs", "tp"),
    P("fs", "tp"),
    P("tp", "fs"),
)


def permuted(mesh):
    return jax.shard_map(
        build(mesh.shape["fs"]),
        mesh=mesh,
        in_specs=SPECS,
        out_specs=P(("rep", "fs", "tp"), None),
        check_vma=False,
    )


def fused(mesh):
    return jax.shard_map(
        functools.partial(block, mesh.shape["fs"]),
        mesh=mesh,
        in_specs=SPECS,
        out_specs=P(("rep", "fs", "tp"), None),
        check_vma=False,
    )


def solution(mesh):
    n_fs, n_rep, n_tp = (mesh.shape[name] for name in ("fs", "rep", "tp"))

    def step(*operands):
        tokens, w_down = operands[0], operands[-1]
        rows = tokens.shape[0] // (n_rep * n_fs * n_tp)
        width = tokens.shape[1] // n_fs
        units = w_down.shape[0] // n_tp
        aligned = (
            (n_rep, n_tp, n_fs % 2) == (2, 2, 0)
            and (rows % (2 * STRIP), width % LANES, units % (4 * STRIP), units % LANES) == (0, 0, 0, 0)
            and tokens.shape[1] % (4 * LANES) == 0
        )
        return (fused if aligned else permuted)(mesh)(*operands)

    return step
```

```python
import functools

import jax
import jax.numpy as jnp
from jax import lax
from jax.experimental import pallas as pl
from jax.experimental.pallas import tpu as pltpu
from jax.sharding import PartitionSpec as P


def rms_scale(matrix, gain):
    values = matrix.astype(jnp.float32)
    factor = lax.rsqrt(jnp.mean(values * values, axis=-1, keepdims=True) + 1e-06)
    return values * factor * gain


def causal_taps(mixed, filters):
    length = mixed.shape[-2]
    padded = jnp.pad(mixed, [(2, 0), (0, 0)])
    return (
        filters[0] * padded[0:length]
        + filters[1] * padded[1 : length + 1]
        + filters[2] * padded[2 : length + 2]
    )


def swap(array, axis):
    return lax.ppermute(array, axis, [(0, 1), (1, 0)])


def half(array, axis, part):
    size = array.shape[axis] // 2
    return lax.dynamic_slice_in_dim(array, part * size, size, axis)


def build(n_fs):
    ring = [(i, (i + 2) % n_fs) for i in range(n_fs)]
    pair = [(i, i ^ 1) for i in range(n_fs)]
    steps = n_fs // 2

    def ring_first(block):
        blocks = []
        for step in range(steps):
            blocks += [block, lax.ppermute(block, "fs", pair)]
            if step < steps - 1:
                block = lax.ppermute(block, "fs", ring)
        return blocks

    def pair_first(block):
        mate = lax.ppermute(block, "fs", pair)
        blocks = []
        for step in range(steps):
            blocks += [block, mate]
            if step < steps - 1:
                block = lax.ppermute(block, "fs", ring)
                mate = lax.ppermute(mate, "fs", ring)
        return blocks

    def on_device(
        tokens, mix_gain, w_bgate, w_cgate, w_value, conv_taps, w_mixout, mlp_gain, w_gate, w_up, w_down
    ):
        rep, fs, tp = (lax.axis_index(name) for name in ("rep", "fs", "tp"))
        width = tokens.shape[1] // n_fs

        def arrival_order(array):
            order = [((fs ^ j) - 2 * s + n_fs) % n_fs for s in range(steps) for j in range(2)]
            return jnp.concatenate(
                [lax.dynamic_slice_in_dim(array, k * width, width, array.ndim - 1) for k in order],
                axis=-1,
            )

        def global_order(array):
            places = []
            for k in range(n_fs):
                j = (fs ^ k) & 1
                places.append((((fs ^ j) - k + n_fs) % n_fs) + j)
            return jnp.concatenate(
                [lax.dynamic_slice_in_dim(array, k * width, width, array.ndim - 1) for k in places],
                axis=-1,
            )

        def sequence(rows):
            other = swap(rows, "tp")
            return jnp.concatenate(
                [jnp.where(tp == 0, rows, other), jnp.where(tp == 0, other, rows)], axis=0
            )

        def both_sequences(rows):
            away = swap(rows, "rep")
            return sequence(rows), sequence(away)

        def chip_sum(partial):
            other = swap(half(partial, 0, 1 - tp), "tp")
            return half(partial, 0, tp).astype(jnp.float32) + other.astype(jnp.float32)

        def project_out(mine, theirs, blocks, group):
            sums = []
            for start in range(0, len(blocks), group):
                weight = jnp.concatenate(blocks[start : start + group], axis=1)
                outs = []
                for rows in (theirs, mine):
                    outs.append(
                        jnp.dot(rows, weight, preferred_element_type=jnp.float32).astype(
                            jnp.bfloat16
                        )
                    )
                away = swap(chip_sum(outs[0]).astype(jnp.bfloat16), "rep")
                sums.append(chip_sum(outs[1]) + away.astype(jnp.float32))
            return jnp.concatenate(sums, axis=1)

        w_in = jnp.concatenate([half(w, 1, rep) for w in (w_bgate, w_cgate, w_value)], axis=1)
        w_gu = jnp.concatenate([half(w, 1, rep) for w in (w_gate, w_up)], axis=1)
        in_blocks = ring_first(w_in)
        out_blocks = ring_first(half(w_mixout, 0, rep))
        upper, lower = jnp.split(w_gu, 2, axis=0)
        gu_blocks = [part for both in zip(pair_first(upper), ring_first(lower)) for part in both]
        down_blocks = ring_first(half(w_down, 0, rep))

        channels = w_in.shape[1] // 3
        taps = lax.dynamic_slice_in_dim(conv_taps, (tp * 2 + rep) * channels, channels, 1)
        local = arrival_order(tokens)

        def mix(normed, weight):
            projected = jnp.dot(normed, weight, preferred_element_type=jnp.float32).astype(
                jnp.bfloat16
            )
            b_proj, c_proj, u_proj = (
                projected[:, k * channels : (k + 1) * channels].astype(jnp.float32)
                for k in range(3)
            )
            return (b_proj * causal_taps(c_proj * u_proj, taps)).astype(jnp.bfloat16)

        mine, theirs = both_sequences(rms_scale(local, arrival_order(mix_gain)).astype(jnp.bfloat16))
        weight = jnp.concatenate(in_blocks, axis=0)
        theirs, mine = mix(theirs, weight), mix(mine, weight)
        mixed = project_out(mine, theirs, out_blocks, 2)
        residual = local.astype(jnp.float32) + mixed

        units = w_gu.shape[1] // 2

        def feed(normed, weight):
            both = jnp.dot(normed, weight, preferred_element_type=jnp.float32)
            return (jax.nn.silu(both[:, :units]) * both[:, units:]).astype(jnp.bfloat16)

        mine, theirs = both_sequences(rms_scale(residual, arrival_order(mlp_gain)).astype(jnp.bfloat16))
        weight = jnp.concatenate(gu_blocks, axis=0)
        theirs, mine = feed(theirs, weight), feed(mine, weight)
        down = project_out(mine, theirs, down_blocks, 2)
        return global_order((residual + 0.5 * down).astype(jnp.bfloat16))

    return on_device


MESH = pl.DeviceIdType.MESH
STRIP = 16
LANES = 128
C, U, B, OUT, *GU, DN = TYPES = range(9)
SHARED = (DN,)


def f32(value):
    return value.astype(jnp.float32)


def mxu(left, right):
    return jnp.dot(left, right, preferred_element_type=jnp.float32)


def kernel(
    n_z,
    tok_hbm, gain_one, wb_hbm, wc_hbm, wu_hbm, taps, wo_hbm, gain_two, wg_hbm, wup_hbm, wd_hbm,
    final,
    wb, wc, wu, wo, wgu, wd,
    raw_gate, raw_up, away,
    tok, normed, convolved, gated, part, theirs, outgo, income, res, normed_two, hidden,
    part_two, theirs_two, outgo_two, income_two,
    tail,
    load_sem, y_send, y_recv, z_send, z_recv, x_send, x_recv, x_each,
    one_send, one_recv, mix_send, mix_recv, mid_send, mid_recv, two_send, two_recv,
):
    rep, fs, tp = (lax.axis_index(name) for name in ("rep", "fs", "tp"))
    z, y = lax.div(fs, 2), lax.rem(fs, 2)
    rows, _ = tok.shape
    sub = rows // 2
    depth = wb_hbm.shape[0]
    channels = wb.shape[1]
    pair_units = wgu.shape[1]
    units = pair_units // 2
    width = wo.shape[2]
    n_fs = 2 * n_z
    core = (rep, fs, 1 - tp)
    mate = (rep, z * 2 + 1 - y, tp)
    twin = (1 - rep, fs, tp)

    def along(position):
        return (rep, position * 2 + y, tp)

    def kth(k):
        near = jnp.minimum(z, n_z - 1 - z)
        longer = jnp.where(z < n_z - 1 - z, 1, -1)
        both = z + longer * (((k + 1) // 2) * (1 if k % 2 == 1 else -1))
        return jnp.where(k <= 2 * near, both, z + longer * (k - near))

    def line(rr, position):
        return position * 2 + (y if rr == 0 else 1 - y)

    def rows_of(t, piece, base):
        if t in (OUT, DN):
            size = (wo, wd)[t == DN].shape[1] // 2
        else:
            size = depth // (2 * len(GU) if t in GU else 2)
        first = base + (2 * size * GU.index(t) if t in GU else 0)
        if piece is None:
            return pl.ds(pl.multiple_of(first, 16), 2 * size)
        return pl.ds(pl.multiple_of(first + piece * size, 16), size)

    def source(t, half, piece=None):
        if t in (OUT, DN):
            ref = (wo_hbm, wd_hbm)[t == DN]
            return ref.at[rows_of(t, piece, half * (ref.shape[0] // 2)), :]
        ref = (wc_hbm, wu_hbm, wb_hbm)[t]
        return ref.at[rows_of(t, piece, 0), pl.ds(pl.multiple_of(half * channels, 128), channels)]

    def slot(t, index, piece=None):
        if t in (OUT, DN):
            return (wo, wd)[t == DN].at[index, rows_of(t, piece, 0), :]
        return (wgu if t in GU else (wc, wu, wb)[t]).at[rows_of(t, piece, index * depth), :]

    def remote(src, dst, send, recv, device):
        return pltpu.make_async_remote_copy(
            src_ref=src, dst_ref=dst, send_sem=send, recv_sem=recv, device_id=device, device_id_type=MESH
        )


    def local(t):
        return pltpu.make_async_copy(source(t, y), slot(t, fs), load_sem.at[t])

    def y_copy(t, index):
        piece = rep if t in SHARED else None
        src = away.at[rows_of(t, piece, 0), :] if t in GU else source(t, 1 - y, piece)
        return remote(src, slot(t, index, piece), y_send.at[t], y_recv.at[t], mate)

    def z_own(t, rr, side):
        index = line(rr, z)
        src = slot(t, index, rep) if rr == 1 or t in GU else source(t, y, rep)
        return remote(
            src, slot(t, index, rep), z_send.at[t], z_recv.at[t, rr, z - (side < 0)], along(z + side)
        )

    def z_fwd(t, rr, position, target):
        place = slot(t, line(rr, position), rep)
        return remote(place, place, z_send.at[t], z_recv.at[t, rr, position - (position > target).astype(jnp.int32)], along(target))

    def x_copy(t, rr, position, piece, own=False):
        place = slot(t, line(rr, position), piece)
        recv = x_each.at[(OUT, DN).index(t), rr, position] if t in (OUT, DN) else x_recv.at[t]
        return remote(place, place, x_send.at[len(TYPES) if own else t], recv, twin)

    def drain(t, pieces, sem):
        if t in (OUT, DN):
            region = (wo, wd)[t == DN].at[pl.ds(0, pieces // 2)]
        else:
            size = depth // (2 * len(GU) if t in GU else 2)
            region = (wgu if t in GU else (wc, wu, wb)[t]).at[pl.ds(0, pieces * size), :]
        pltpu.make_async_copy(region, region, sem).wait()

    def z_each(t, rr, act):
        for side in (-1, 1):

            @pl.when(jnp.logical_and(z + side >= 0, z + side < n_z))
            def _():
                act(z_own(t, rr, side))

    def start_own(t, rr):
        if rr == 1:
            y_copy(t, line(1, z)).wait_recv()
            if t in SHARED:
                x_copy(t, 1, z, rep, True).start()
        z_each(t, rr, lambda copy: copy.start())

    inner = jnp.minimum(z, n_z - 1 - z) > 0
    outer = jnp.logical_not(inner)

    def relay(t, rr, k):
        position = kth(k)
        onward = z + jnp.where(position < z, 1, -1)
        z_fwd(t, rr, position, z).wait_recv()

        @pl.when(jnp.logical_and(onward >= 0, onward < n_z))
        def _():
            z_fwd(t, rr, position, onward).start()

        x_copy(t, rr, position, rep).start()

    def relay_if(where, t, rr, ks):
        @pl.when(where)
        def _():
            for k in ks:
                relay(t, rr, k)

    beyond = range(3, n_z)

    def x_wait(t, pairs):
        for rr, k in pairs:
            x_copy(t, rr, kth(k), 1 - rep).wait_recv()

    def x_all(t):
        drain(t, 2 * (n_z - 1), x_recv.at[t])


    def half_rows(which, first=0, count=None):
        return pl.ds(pl.multiple_of(which * rows + first, 16), rows if count is None else count)

    def core_copy(src, dst, sems, place, leave=None):
        return remote(src, dst, sems[0].at[place if leave is None else leave], sems[1].at[place], core)

    def mate_copy(src, dst, sems, place, leave=None):
        return remote(src, dst, sems[0].at[place if leave is None else leave], sems[1].at[place], mate)

    one, mix, mid, two = (one_send, one_recv), (mix_send, mix_recv), (mid_send, mid_recv), (two_send, two_recv)
    mine, other = half_rows(tp), half_rows(1 - tp)


    barrier = pltpu.get_barrier_semaphore()
    for device in (core, mate, twin):
        pl.semaphore_signal(barrier, inc=1, device_id=device, device_id_type=MESH)
    neighbours = 3
    for side in (-1, 1):
        inside = jnp.logical_and(z + side >= 0, z + side < n_z)
        neighbours += inside.astype(jnp.int32)

        @pl.when(inside)
        def _(side=side):
            pl.semaphore_signal(barrier, inc=1, device_id=along(z + side), device_id_type=MESH)

    raw = [
        pltpu.make_async_copy(src, dst, load_sem.at[place])
        for src, dst, place in ((tok_hbm, tok, GU[0]), (wg_hbm, raw_gate, GU[1]), (wup_hbm, raw_up, len(TYPES)))
    ]
    raw[0].start()
    pl.semaphore_wait(barrier, neighbours)
    for t in (C, U, B):
        y_copy(t, fs).start()
    for t in (C, U, B):
        start_own(t, 0)
    for copy in raw[1:]:
        copy.start()
    for t in (C, U, B, OUT, DN):
        local(t).start()
    raw[0].wait()

    @pl.loop(0, rows // STRIP)
    def _(i):
        at = pl.ds(pl.multiple_of(i * STRIP, STRIP), STRIP)
        values = f32(tok[at, :])
        factor = lax.rsqrt(jnp.mean(values * values, axis=-1, keepdims=True) + 1e-06)
        normed[0, pl.ds(pl.multiple_of(tp * rows + i * STRIP, STRIP), STRIP), :] = (
            values * factor * gain_one[...]
        ).astype(jnp.bfloat16)

    one_core = core_copy(normed.at[0, mine, :], normed.at[0, mine, :], one, 0)
    one_mate = mate_copy(normed.at[0, mine, :], normed.at[1, mine, :], one, 1)
    one_pass = core_copy(normed.at[1, mine, :], normed.at[1, mine, :], one, 2)
    y_copy(OUT, fs).start()
    one_core.start()
    one_mate.start()

    def relays(types, rr, k):
        for t in types:
            relay(t, rr, k)

    three = (C, U, B)
    relays(three, 0, 1)
    start_own(C, 1)
    for copy in raw[1:]:
        copy.wait()

    @pl.loop(0, depth // STRIP)
    def _(i):
        at = pl.ds(pl.multiple_of(i * STRIP, STRIP), STRIP)
        here = pl.ds(pl.multiple_of(fs * depth + i * STRIP, STRIP), STRIP)
        gate, up = f32(raw_gate[at, :]), f32(raw_up[at, :])
        for half in range(2):
            cut = slice(half * units, (half + 1) * units)
            both = jnp.concatenate([gate[:, cut], up[:, cut]], axis=1).astype(jnp.bfloat16)

            @pl.when(y == half)
            def _(both=both):
                wgu[here, :] = both

            @pl.when(y != half)
            def _(both=both):
                away[at, :] = both

    for t in (*GU, DN):
        y_copy(t, fs).start()


    my_taps = pl.ds(pl.multiple_of((tp * 2 + y) * channels, 128), channels)

    def convolve(seq, half):
        at = pl.ds(half * rows, rows)
        left = normed[seq, at, :]
        mixed = f32(mxu(left, wc[...]).astype(jnp.bfloat16)) * f32(mxu(left, wu[...]).astype(jnp.bfloat16))
        row = lax.broadcasted_iota(jnp.int32, mixed.shape, 0)
        before = [jnp.zeros((1, channels), jnp.float32)] * 2 if half == 0 else [tail[0:1, :], tail[1:2, :]]
        back_one = jnp.where(row == 0, before[1], pltpu.roll(mixed, 1, 0))
        back_two = jnp.where(row == 0, before[0], jnp.where(row == 1, before[1], pltpu.roll(mixed, 2, 0)))
        if half == 0:
            tail[0:2, :] = mixed[rows - 2 : rows, :]
        convolved[seq, at, :] = (
            taps[0:1, my_taps] * back_two + taps[1:2, my_taps] * back_one + taps[2:3, my_taps] * mixed
        )

    def gate_out(seq, half):
        at = pl.ds(half * rows, rows)
        b_proj = f32(mxu(normed[seq, at, :], wb[...]).astype(jnp.bfloat16))
        gated[seq, at, :] = (b_proj * convolved[seq, at, :]).astype(jnp.bfloat16)

    arrivals = sorted((max(k, 2), rr, k) for rr in range(2) for k in range(1, n_z))
    for place, (_, rr, k) in enumerate(arrivals[1:]):
        if place == len(arrivals) - 3:
            start_own(OUT, 0)
        relays(three, rr, k)
        if place == 0:
            start_own(U, 1)
            start_own(B, 1)
    start_own(OUT, 1)
    relay(OUT, 0, 1)
    relay(OUT, 1, 1)
    relay_if(inner, OUT, 0, [2])
    relay_if(inner, OUT, 1, [2])
    one_mate.wait_recv()
    one_pass.start()
    for t in (C, U):
        local(t).wait()
        x_all(t)
    core_copy(normed.at[1, other, :], normed.at[1, other, :], one, 2).wait_recv()

    halves = [pl.ds(i * sub, sub) for i in range(2)]

    def piece(which, i):
        return half_rows(which, i * sub, sub)

    def mix_core(index, i):
        return core_copy(
            part.at[index, 1, piece(1 - tp, i), :], theirs.at[index, 1, halves[i], :], mix, index * 4 + i, 0
        )

    def mix_mate(index, i):
        return mate_copy(outgo.at[index, halves[i], :], income.at[index, halves[i], :], mix, index * 4 + 2 + i, 1)

    def mix_own(index):
        return core_copy(part.at[index, 0, other, :], theirs.at[index, 0], mix, 4 * n_fs, 2)

    def project_out(index, i):
        right = wo[index]
        for which in (1 - tp, tp):
            at = piece(which, i)
            part[index, 1, at, :] = mxu(gated[1, at, :], right).astype(jnp.bfloat16)
            if which is not tp:
                mix_core(index, i).start()

    def project_own(index):
        right = wo[index]
        part[index, 0, other, :] = mxu(gated[0, other, :], right).astype(jnp.bfloat16)
        mix_own(index).start()
        part[index, 0, mine, :] = mxu(gated[0, mine, :], right).astype(jnp.bfloat16)

    def send_sum(index, i):
        mix_core(index, i).wait_recv()
        outgo[index, halves[i], :] = (
            f32(part[index, 1, piece(tp, i), :]) + f32(theirs[index, 1, halves[i], :])
        ).astype(jnp.bfloat16)
        mix_mate(index, i).start()

    order = [line(rr, kth(k)) for k in range(n_z) for rr in range(2)]

    def mix_out(places, i):
        places = list(places)
        for place in places:
            if i == 0 and place > 1:
                x_wait(OUT, [(place % 2, place // 2)])
            project_out(order[place], i)
            if place > places[0]:
                send_sum(order[place - 1], i)
        send_sum(order[places[-1]], i)

    convolve(1, 0)
    relay_if(outer, OUT, 0, [2])
    relay_if(inner, OUT, 0, beyond)
    convolve(1, 1)
    relay_if(outer, OUT, 1, [2])
    relay_if(inner, OUT, 1, beyond)
    for t in GU:
        start_own(t, 0)
    local(B).wait()
    x_all(B)
    gate_out(1, 0)
    gate_out(1, 1)
    local(OUT).wait()
    mix_out(range(2), 0)
    relay_if(outer, OUT, 0, beyond)
    mix_out(range(2, 4), 0)
    relay_if(outer, OUT, 1, beyond)
    for t in GU:
        start_own(t, 1)
    core_copy(normed.at[0, other, :], normed.at[0, other, :], one, 0).wait_recv()
    todo = [(t, rr, k) for k in range(1, n_z) for rr in range(2) for t in GU]
    todo = [(inner, todo[::-1]), (outer, todo[::-1])]

    def pump(*counts):
        for (where, left), count in zip(todo, counts):
            items = [left.pop() for _ in range(min(count, len(left)))]

            @pl.when(where)
            def _(items=items):
                for item in items:
                    relay(*item)

    mix_out(range(4), 1)
    pump(1, 1)
    mix_out(range(4, 6), 0)
    pump(1, 1)
    mix_out(range(6, n_fs), 0)
    pump(1, 1)
    mix_out(range(4, n_fs), 1)
    pump(2, 2)
    convolve(0, 0)
    pump(1, 1)
    convolve(0, 1)
    pump(2, 1)
    gate_out(0, 0)
    gate_out(0, 1)
    pump(3, 1)
    for index in order:
        project_own(index)

    def add_up(index, i):
        mix_mate(index, i).wait_recv()
        at, cols = halves[i], pl.ds(pl.multiple_of(index * width, 128), width)
        res[at, cols] = f32(tok[at, cols]) + (
            (f32(part[index, 0, piece(tp, i), :]) + f32(theirs[index, 0, at, :])) + f32(income[index, at, :])
        )

    strips = sub // STRIP

    def mid_core(which, i):
        return core_copy(normed_two.at[0, piece(which, i), :], normed_two.at[0, piece(which, i), :], mid, i)

    def mid_mate(i):
        return mate_copy(normed_two.at[0, piece(tp, i), :], normed_two.at[1, piece(tp, i), :], mid, 2 + i)

    def mid_pass(which, i):
        return core_copy(normed_two.at[1, piece(which, i), :], normed_two.at[1, piece(which, i), :], mid, 4 + i)

    def norm_two(i, relays_after):
        if i == 0:
            pltpu.make_async_copy(outgo, outgo, mix_recv.at[4 * n_fs]).wait()
        for place, index in enumerate(order):
            add_up(index, i)
            if place in relays_after:
                pump(1, 1)

        @pl.loop(0, strips)
        def _(j):
            first = i * sub + j * STRIP
            at = pl.ds(pl.multiple_of(first, STRIP), STRIP)
            values = res[at, :]
            factor = lax.rsqrt(jnp.mean(values * values, axis=-1, keepdims=True) + 1e-06)
            normed_two[0, half_rows(tp, first, STRIP), :] = (values * factor * gain_two[...]).astype(jnp.bfloat16)

        mid_mate(i).start()
        mid_core(tp, i).start()

    pump(5, 1)

    def start_down(where):
        @pl.when(where)
        def _():
            for rr in range(2):
                z_each(DN, rr, lambda copy: copy.start())

    y_copy(DN, line(1, z)).wait_recv()
    start_down(outer)
    norm_two(0, [4])
    pump(1, 1)
    norm_two(1, range(n_fs - 1))
    rest = len(GU) * 2 * (n_z - 1)
    pump(rest, rest)
    start_down(inner)
    x_copy(DN, 1, z, rep, True).start()
    for k in (1, 2):
        for rr in range(2):
            relay_if(inner, DN, rr, [k])


    def feed(seq, at):
        both = mxu(normed_two[seq, at, :], wgu[...])
        gate, up = both[:, :units], both[:, units:]
        hidden[seq, at, :] = (gate / (1.0 + jnp.exp(-gate)) * up).astype(jnp.bfloat16)

    def two_core(index, i):
        return core_copy(
            part_two.at[index, 1, piece(1 - tp, i), :], theirs_two.at[index, 1, halves[i], :], two, index * 4 + i, 0
        )

    def two_mate(index, i):
        return mate_copy(
            outgo_two.at[index, halves[i], :], income_two.at[index, halves[i], :], two, index * 4 + 2 + i, 1
        )

    def two_own(index):
        return core_copy(part_two.at[index, 0, other, :], theirs_two.at[index, 0], two, 4 * n_fs, 2)

    def down(index, i):
        right = wd[index]
        for which in (1 - tp, tp):
            at = piece(which, i)
            part_two[index, 1, at, :] = mxu(hidden[1, at, :], right).astype(jnp.bfloat16)
        two_core(index, i).start()

    def add_cores(index, i):
        two_core(index, i).wait_recv()
        outgo_two[index, halves[i], :] = (
            f32(part_two[index, 1, piece(tp, i), :]) + f32(theirs_two[index, 1, halves[i], :])
        ).astype(jnp.bfloat16)
        two_mate(index, i).start()

    def down_own(index):
        right = wd[index]
        for at in (other, mine):
            part_two[index, 0, at, :] = mxu(hidden[0, at, :], right).astype(jnp.bfloat16)
        two_own(index).start()

    behind = []

    def step(place, i):
        down(order[place], i)
        if behind:
            add_cores(*behind.pop())
        behind.append((order[place], i))

    def flush():
        while behind:
            add_cores(*behind.pop())

    def both_down(place):
        x_wait(DN, [(place % 2, place // 2)])
        step(place, 0)
        step(place, 1)

    mid_mate(0).wait_recv()
    mid_pass(tp, 0).start()
    for rr in range(2):
        relay_if(inner, DN, rr, beyond)
    for t in GU:
        x_all(t)
    relay_if(outer, DN, 0, [1])
    feed(1, piece(tp, 0))
    relay_if(outer, DN, 1, [1])
    mid_pass(1 - tp, 0).wait_recv()
    feed(1, piece(1 - tp, 0))
    local(DN).wait()
    if DN in SHARED:
        x_wait(DN, [(1, 0)])
    step(0, 0)
    step(1, 0)
    flush()
    relay_if(outer, DN, 0, [2])
    mid_mate(1).wait_recv()
    mid_pass(tp, 1).start()
    feed(1, piece(tp, 1))
    mid_pass(1 - tp, 1).wait_recv()
    feed(1, piece(1 - tp, 1))
    step(0, 1)
    step(1, 1)
    flush()
    relay_if(outer, DN, 1, [2])
    both_down(2)
    both_down(3)
    flush()
    feed(0, mine)
    both_down(4)
    relay_if(outer, DN, 0, beyond)
    both_down(5)
    flush()
    mid_core(1 - tp, 0).wait_recv()
    mid_core(1 - tp, 1).wait_recv()
    feed(0, other)
    relay_if(outer, DN, 1, beyond)
    for place in range(6, n_fs):
        both_down(place)
        flush()
        down_own(order[place - 6])
    for place in range(n_fs - 6, n_fs):
        down_own(order[place])
    pltpu.make_async_copy(outgo_two, outgo_two, two_recv.at[4 * n_fs]).wait()
    for index in order:
        for i in range(2):
            two_mate(index, i).wait_recv()
        cols = pl.ds(pl.multiple_of(index * width, 128), width)
        total = (f32(part_two[index, 0, mine, :]) + f32(theirs_two[index, 0])) + f32(income_two[index])
        final[:, cols] = (res[:, cols] + 0.5 * total).astype(jnp.bfloat16)


    for t in TYPES:
        y_copy(t, fs).wait_send()
        drain(t, 2 * (n_z - 1), x_send.at[t])

        @pl.when(inner)
        def _(t=t):
            drain(t, 4 + 2 * (n_z - 1), z_send.at[t])

        @pl.when(outer)
        def _(t=t):
            drain(t, 2, z_send.at[t])

        if t in SHARED:
            x_copy(t, 1, z, rep, True).wait_send()
    for send, whole in ((mix_send, outgo), (two_send, outgo_two)):
        for place in range(3):
            pltpu.make_async_copy(whole, whole, send.at[place]).wait()
    sent = [one_core, one_mate, one_pass]
    sent += [make for i in range(2) for make in (mid_core(tp, i), mid_mate(i), mid_pass(tp, i))]
    for copy in sent:
        copy.wait_send()


def block(
    n_fs, tokens, mix_gain, w_bgate, w_cgate, w_value, conv_taps, w_mixout, mlp_gain, w_gate, w_up, w_down
):
    rows, dim = tokens.shape
    depth, channels = w_bgate.shape[0], w_bgate.shape[1] // 2
    units = w_gate.shape[1] // 2
    width = w_mixout.shape[1]
    n_z = n_fs // 2
    bf16 = jnp.bfloat16
    hbm = pl.BlockSpec(memory_space=pl.ANY)
    vmem = pl.BlockSpec(memory_space=pltpu.VMEM)
    dma = pltpu.SemaphoreType.DMA
    return pl.pallas_call(
        functools.partial(kernel, n_z),
        out_shape=pltpu.VMEM(tokens.shape, tokens.dtype),
        in_specs=[hbm, vmem, hbm, hbm, hbm, vmem, hbm, vmem, hbm, hbm, hbm],
        out_specs=vmem,
        scratch_shapes=[
            *[pltpu.VMEM((n_fs * depth, channels), bf16)] * 3,
            pltpu.VMEM((n_fs, w_mixout.shape[0] // 2, width), bf16),
            pltpu.VMEM((n_fs * depth, 2 * units), bf16),
            pltpu.VMEM((n_fs, w_down.shape[0] // 2, width), bf16),
            *[pltpu.VMEM((depth, 2 * units), bf16)] * 3,
            pltpu.VMEM((rows, dim), bf16),
            pltpu.VMEM((2, 2 * rows, dim), bf16),
            pltpu.VMEM((2, 2 * rows, channels), jnp.float32),
            pltpu.VMEM((2, 2 * rows, channels), bf16),
            pltpu.VMEM((n_fs, 2, 2 * rows, width), bf16),
            pltpu.VMEM((n_fs, 2, rows, width), bf16),
            pltpu.VMEM((n_fs, rows, width), bf16),
            pltpu.VMEM((n_fs, rows, width), bf16),
            pltpu.VMEM((rows, dim), jnp.float32),
            pltpu.VMEM((2, 2 * rows, dim), bf16),
            pltpu.VMEM((2, 2 * rows, units), bf16),
            pltpu.VMEM((n_fs, 2, 2 * rows, width), bf16),
            pltpu.VMEM((n_fs, 2, rows, width), bf16),
            pltpu.VMEM((n_fs, rows, width), bf16),
            pltpu.VMEM((n_fs, rows, width), bf16),
            pltpu.VMEM((8, channels), jnp.float32),
            dma((len(TYPES) + 1,)),
            *[dma((len(TYPES),))] * 3,
            dma((len(TYPES), 2, n_z - 1)),
            dma((len(TYPES) + 1,)),
            dma((len(TYPES),)),
            dma((2, 2, n_z)),
            *[dma((3,))] * 2,
            *[dma((3,)), dma((4 * n_fs + 1,))],
            *[dma((6,))] * 2,
            *[dma((3,)), dma((4 * n_fs + 1,))],
        ],
        compiler_params=pltpu.CompilerParams(
            collective_id=0, has_side_effects=True, vmem_limit_bytes=64_500_000
        ),
    )(
        tokens, mix_gain[None], w_bgate, w_cgate, w_value, conv_taps, w_mixout, mlp_gain[None], w_gate, w_up, w_down
    )


SPECS = (
    P(("rep", "fs", "tp"), None),
    P(),
    P("fs", "tp"),
    P("fs", "tp"),
    P("fs", "tp"),
    P(),
    P("tp", "fs"),
    P(),
    P("fs", "tp"),
    P("fs", "tp"),
    P("tp", "fs"),
)


def permuted(mesh):
    return jax.shard_map(
        build(mesh.shape["fs"]),
        mesh=mesh,
        in_specs=SPECS,
        out_specs=P(("rep", "fs", "tp"), None),
        check_vma=False,
    )


def fused(mesh):
    return jax.shard_map(
        functools.partial(block, mesh.shape["fs"]),
        mesh=mesh,
        in_specs=SPECS,
        out_specs=P(("rep", "fs", "tp"), None),
        check_vma=False,
    )


def solution(mesh):
    n_fs, n_rep, n_tp = (mesh.shape[name] for name in ("fs", "rep", "tp"))

    def step(*operands):
        tokens, w_down = operands[0], operands[-1]
        rows = tokens.shape[0] // (n_rep * n_fs * n_tp)
        width = tokens.shape[1] // n_fs
        units = w_down.shape[0] // n_tp
        aligned = (
            (n_rep, n_tp, n_fs % 2) == (2, 2, 0)
            and (rows % (2 * STRIP), width % LANES, units % (4 * STRIP), units % LANES) == (0, 0, 0, 0)
            and tokens.shape[1] % (4 * LANES) == 0
        )
        return (fused if aligned else permuted)(mesh)(*operands)

    return step
```
